32 devices in a mesh: grp: 2 (over y), sp: 4 (over z), dp: 4 (over x, core).
Axes of the slice: x: 2, y: 2, z: 4, core: 2. Of those that a mesh axis runs over, the one named last changes fastest.
Arguments:
- queries: bfloat16 [8, 512, 16, 192], P(('grp', 'dp'), 'sp'), parts along dimension 0, may hold values from -41 to 41
- kv_latent: bfloat16 [8, 512, 512], P(('grp', 'dp'), 'sp'), parts along dimension 0, may hold values from -6 to 6
- rope_key: bfloat16 [8, 512, 64], P(('grp', 'dp'), 'sp'), parts along dimension 0, may hold values from -5.1 to 5.1
- kv_gain: float32 [512], replicated, may hold values from 0.1 to 1.9
- kv_weight: bfloat16 [512, 4096], P('dp', 'sp'), may hold values from -0.25 to 0.25
- out_weight: bfloat16 [2048, 2048], P(None, 'dp'), may hold values from -1 to 1
Outputs:
- mixed: bfloat16 [8, 512, 2048], P(('grp', 'dp'), 'sp'), parts along dimension 0
The draws below stay inside these ranges and needn't reach their ends.
There are 2 independent parts, one for each index of `grp`. The reference program is written for one: setup_inputs(seed, part) draws one part's arguments, and reference() takes and returns one part's arrays. A program takes and returns all parts, laid end to end along the dimension named above; an argument that names none is the same for every part. Nothing has to cross between parts.
All inputs are finite; a program needn't handle non-finite values.
Results may differ from the reference program's by a relative error of at most 0.0075.
Values may be sent and summed in bfloat16 or wider, within the bound.
A program may use at most 64 MiB of HBM per device.

```python
import jax
import jax.numpy as jnp
from jax import lax

D = 2048
H = 16
KL = 512
NOPE = 128
ROPE = 64
VD = 128
LEN = 512
SEQS = 4


def paired_draw(key):
    base = jax.random.fold_in(key, 41)
    first_key, second_key = jax.random.split(base)
    query_shape = (SEQS, LEN, H, NOPE + ROPE)
    shared = jnp.clip(jax.random.normal(first_key, (SEQS, LEN, ROPE), jnp.float32), -5.0, 5.0)
    query = jnp.clip(jax.random.normal(second_key, query_shape, jnp.float32), -5.0, 5.0)
    return (query, shared)


def draw_queries(key, part):
    return paired_draw(key)[0].astype(jnp.bfloat16)


def draw_rope_key(key, part):
    return paired_draw(key)[1].astype(jnp.bfloat16)


def levels(stream_key, shape, cuts, smallest, high):
    level, own = 1.0, jax.random.fold_in(stream_key, 6)
    for position, parts in cuts:
        draws = jnp.exp(jax.random.uniform(jax.random.fold_in(own, position), (parts,), jnp.float32, smallest / len(cuts), high / len(cuts)))
        level = level * jnp.repeat(draws, shape[position] // parts).reshape([-1 if axis == position else 1 for axis in range(len(shape))])
    return level


def scatter_about(own_key, shape, scale, bound, cuts=(), kind=jnp.bfloat16):
    gain = levels(own_key, shape, cuts, -0.22, 0.18) if cuts else 1.0
    values = jax.random.normal(own_key, shape, jnp.float32) * scale * gain
    return jnp.minimum(jnp.maximum(values, -bound), bound).astype(kind)


def setup_inputs(seed: int = 0, part: int = 0) -> dict:
    seeds = jax.random.split(jax.random.key(seed), 7)
    part_splits = jax.random.split(jax.random.fold_in(seeds[6], part), 7)
    return {
        "queries": draw_queries(jax.random.fold_in(jax.random.fold_in(seeds[6], part), 71), part),
        "kv_latent": scatter_about(part_splits[1], (SEQS, LEN, KL), 1.0, 6.0, ((0, 4), (1, 4))),
        "rope_key": draw_rope_key(jax.random.fold_in(jax.random.fold_in(seeds[6], part), 71), part),
        "kv_gain": jnp.clip(1.0 + 0.18 * jax.random.normal(seeds[3], (KL,), jnp.float32), 0.1, 1.9),
        "kv_weight": scatter_about(seeds[4], (KL, H * (NOPE + VD)), KL ** -0.5, 0.25, ((0, 4), (1, 4))),
        "out_weight": scatter_about(seeds[5], (H * VD, D), 32 ** -0.5, 1.0, ((1, 4),)),
    }


def rotate(values, positions):
    half = values.shape[-1] // 2
    inverse = jnp.power(10000.0, -jnp.arange(half, dtype=jnp.float32) * 2.0 / values.shape[-1])
    angle = positions.astype(jnp.float32)[..., None] * inverse
    first = values[..., :half].astype(jnp.float32)
    second = values[..., half:].astype(jnp.float32)
    cosine = jnp.cos(angle)
    sine = jnp.sin(angle)
    return jnp.concatenate([first * cosine - second * sine, first * sine + second * cosine], axis=-1)

def attend(query_rot, key_value, key_rot):
    length, heads = (query_rot.shape[0], query_rot.shape[1])
    nope = query_rot.shape[2] - key_rot.shape[1]
    scale = query_rot.shape[2] ** (-0.5)
    content = key_value[:, :, :nope]
    values = key_value[:, :, nope:].astype(jnp.float32)
    shared = jnp.broadcast_to(key_rot[:, None, :], (length, heads, key_rot.shape[1]))
    keys = jnp.concatenate([content, shared], axis=-1).astype(jnp.float32)
    block = min(512, length)
    blocks = query_rot.reshape(length // block, block, heads, query_rot.shape[2])
    key_pos = jnp.arange(length, dtype=jnp.int32)

    def one_block(item):
        query_block, index = item
        scores = jnp.einsum('qhd,khd->hqk', query_block.astype(jnp.float32), keys) * scale
        query_pos = index * block + jnp.arange(block, dtype=jnp.int32)
        kept = query_pos[:, None] >= key_pos[None, :]
        scores = jnp.where(kept[None], scores, -jnp.inf)
        top = lax.optimization_barrier(jnp.max(scores, axis=-1, keepdims=True))
        expo = jnp.exp(scores - top)
        probs = (expo / lax.optimization_barrier(jnp.sum(expo, axis=-1, keepdims=True))).astype(jnp.bfloat16)
        return jnp.einsum('hqk,khd->qhd', probs.astype(jnp.float32), values).astype(jnp.bfloat16)
    result = lax.map(one_block, (blocks, jnp.arange(length // block, dtype=jnp.int32)))
    return result.reshape(length, heads, values.shape[2])

def reference(queries, kv_latent, rope_key, kv_gain, kv_weight, out_weight):
    positions = jnp.arange(LEN, dtype=jnp.int32)

    def one_sequence(item):
        query, latent, shared = item
        latent32 = latent.astype(jnp.float32)
        latent_n = (latent32 * lax.rsqrt(lax.optimization_barrier(jnp.mean(latent32 * latent32, axis=-1, keepdims=True)) + 1e-06) * kv_gain).astype(jnp.bfloat16)
        key_value = jnp.dot(latent_n, kv_weight, preferred_element_type=jnp.float32).astype(jnp.bfloat16)
        key_value = key_value.reshape(LEN, H, NOPE + VD)
        key_rot = rotate(shared, positions).astype(jnp.bfloat16)
        turned = rotate(query[:, :, NOPE:], positions[:, None])
        query_rot = jnp.concatenate([query[:, :, :NOPE].astype(jnp.float32), turned], axis=-1).astype(jnp.bfloat16)
        attended = attend(query_rot, key_value, key_rot).reshape(LEN, H * VD)
        return jnp.dot(attended, out_weight, preferred_element_type=jnp.float32).astype(jnp.bfloat16)
    return lax.map(one_sequence, (queries, kv_latent, rope_key))
```

```python
import functools
import math

import jax
import jax.numpy as jnp
import numpy as np
from jax import lax
from jax.experimental import pallas as pl
from jax.experimental.pallas import tpu as pltpu
from jax.sharding import PartitionSpec as P

NOPE = 128
VD = 128
LANES = 128
CORES = 2
UNITS = 16
LEAD = 3
LAG = 3
SPLIT = 2
VARIANTS = 4
MESH = pl.DeviceIdType.MESH


def rotation_table(length, rope):
    half = rope // 2
    inverse = np.power(10000.0, -np.arange(half) * 2.0 / rope).astype(np.float32)
    angle = inverse[:, None] * np.arange(length, dtype=np.float32)[None, :]
    return np.stack([np.cos(angle), np.sin(angle)]).astype(np.float32)


def kernel(
    n, g, nx, p, hn, rope, scale, sub,
    q_ref, latent_ref, key_ref, gain_ref, table_ref, kvw_ref, w_ref, out_ref,
    qbuf, lat, rkey, shared, kvw, wfull, attout, attin, acc, latin, keyin, gain, table,
    loc, l_s, l_r, r_s, r_r, q_s, q_r, kz_s, kz_r, a_s, a_r,
    kx_s, kx_r, ky_s, ky_r, kc_s, kc_r, ko_s, ko_r,
    wx_s, wx_r, wy_s, wy_r, wc_s, wc_r, wo_s, wo_r,
):
    me = lax.axis_index("sp")
    y = lax.axis_index("grp")
    dp = lax.axis_index("dp")
    x, c = dp // CORES, dp % CORES
    b, r = lax.div(me, p), lax.rem(me, p)
    m = n // p
    ndp = nx * CORES
    tok, latw = latent_ref.shape
    half = rope // 2
    rrows = rkey.shape[1]
    krows = kvw_ref.shape[0]
    kh = krows // g
    cols = w_ref.shape[1]
    kd = hn * VD
    part = kd // g
    crow = part // sub
    units = n * sub
    length = n * tok
    wide = NOPE + VD

    def chip(xx, cc):
        return {"dp": xx * CORES + cc}

    partner = chip(x, 1 - c)

    def remote(src, dst, ss, rs, dev):
        return pltpu.make_async_remote_copy(
            src_ref=src, dst_ref=dst, send_sem=ss, recv_sem=rs, device_id=dev, device_id_type=MESH
        )

    def span(start, size):
        return pl.ds(pl.multiple_of(start, size), size)

    def mate(s):
        return lax.rem(r + s, p)

    def group(o):
        return lax.rem(b + o, m)

    def xs(o):
        return lax.rem(x + nx - o, nx) * CORES + c

    get_lat = pltpu.make_async_copy(latent_ref, latin, loc.at[0])
    get_key = pltpu.make_async_copy(key_ref, keyin, loc.at[1])
    get_gain = pltpu.make_async_copy(gain_ref, gain, loc.at[2])
    get_table = pltpu.make_async_copy(table_ref.at[:, :, span(b * (p * tok), p * tok)], table, loc.at[3])
    own_k = pltpu.make_async_copy(kvw_ref, kvw.at[b, span(dp * krows, krows)], loc.at[4])
    own_w = pltpu.make_async_copy(w_ref, wfull.at[dp], loc.at[5])

    def own_q(i):
        return pltpu.make_async_copy(q_ref.at[span((r + p * i) * hn, hn)], qbuf.at[r, i], loc.at[6 + i])

    for copy in (get_lat, get_key, get_gain, get_table):
        copy.start()

    barrier = pltpu.get_barrier_semaphore()
    for o in range(1, n):
        pl.semaphore_signal(barrier, 1, device_id={"sp": lax.rem(me + o, n)}, device_id_type=MESH)
    for o in range(1, nx):
        pl.semaphore_signal(barrier, 1, device_id=chip(lax.rem(x + o, nx), c), device_id_type=MESH)
    for o in range(1, g):
        pl.semaphore_signal(barrier, 1, device_id={"grp": lax.rem(y + o, g)}, device_id_type=MESH)
    pl.semaphore_signal(barrier, 1, device_id=partner, device_id_type=MESH)

    own_k.start()
    for i in range(m):
        own_q(i).start()
    own_w.start()

    def turned(values, cosine, sine):
        first, second = values[:half].astype(jnp.float32), values[half:].astype(jnp.float32)
        return first * cosine - second * sine, first * sine + second * cosine

    get_lat.wait()
    get_gain.wait()
    latent = latin[...].astype(jnp.float32)
    square = jnp.mean(latent * latent, axis=-1, keepdims=True)
    lat[span(me * tok, tok), :] = (latent * lax.rsqrt(square + 1e-06) * gain[...]).astype(jnp.bfloat16)
    get_key.wait()
    get_table.wait()
    mine = span(r * tok, tok)
    first, second = turned(keyin[...], table[0, :, mine], table[1, :, mine])
    both = jnp.concatenate([first, second], axis=0).astype(jnp.bfloat16)
    for f in range(rope // rrows):
        rkey[me, :, f * tok : (f + 1) * tok] = both[f * rrows : (f + 1) * rrows]

    pl.semaphore_wait(barrier, (n - 1) + (nx - 1) + (g - 1) + 1)

    def kz_copy(o):
        return remote(
            kvw_ref, kvw.at[b, span(dp * krows, krows)], kz_s.at[o - 1], kz_r.at[o - 1],
            {"sp": group(o) * p + r},
        )

    def lat_copies(o):
        to = {"sp": lax.rem(me + o, n)}
        rows = span(me * tok, tok)
        return (
            remote(lat.at[rows], lat.at[rows], l_s.at[o - 1], l_r.at[o - 1], to),
            remote(rkey.at[me], rkey.at[me], r_s.at[o - 1], r_r.at[o - 1], to),
        )

    def lat_sent(o):
        return lax.rem(me + o, n) >= b * p

    def lat_taken(o):
        return lax.rem(me + n - o, n) < (b + 1) * p

    def q_copy(s, e):
        t, i = mate(s), group(e)
        return remote(
            q_ref.at[span((t + p * i) * hn, hn)], qbuf.at[r, i], q_s.at[s - 1, i], q_r.at[s - 1, i],
            {"sp": b * p + t},
        )

    def a_copy(s, i, h):
        t = mate(s)
        return remote(
            attout.at[i, t, h], attin.at[r, i, h], a_s.at[s - 1, i, h], a_r.at[s - 1, i, h],
            {"sp": b * p + t},
        )

    def k_rows(i, d, q):
        return kvw.at[i, span(d * krows + q * kh, kh)]

    def k_x(o, e):
        i = group(e)
        src = kvw_ref.at[span(y * kh, kh)] if e == 0 else k_rows(i, dp, y)
        return remote(
            src, k_rows(i, dp, y), kx_s.at[o - 1, e], kx_r.at[o - 1, e], chip(lax.rem(x + o, nx), c)
        )

    def k_y(o, q, e):
        ref = k_rows(group(e), xs(o), y)
        return remote(
            ref, ref, ky_s.at[o - 1, q - 1, e], ky_r.at[o - 1, q - 1, e], {"grp": lax.rem(y + q, g)}
        )

    def k_c(o, q, e):
        ref = k_rows(group(e), xs(o), lax.rem(y + g - q, g))
        return remote(ref, ref, kc_s.at[o - 1, q, e], kc_r.at[o - 1, q, e], partner)

    def k_own(e):
        dst = kvw.at[group(e), span(dp * krows, krows)]
        return remote(kvw_ref if e == 0 else dst, dst, ko_s.at[e], ko_r.at[e], partner)

    def place(k):
        return lax.rem(r + k % p, p), group(k // p)

    def w_rows(yy, u):
        q, i = place(u // sub)
        return span((q + p * i) * kd + yy * part + (u % sub) * crow, crow)

    def w_x(o, u):
        rows = w_rows(y, u)
        return remote(
            w_ref.at[rows], wfull.at[dp, rows], wx_s.at[o - 1, u], wx_r.at[o - 1, u],
            chip(lax.rem(x + o, nx), c),
        )

    def w_y(o, q, u):
        ref = wfull.at[xs(o), w_rows(y, u)]
        return remote(
            ref, ref, wy_s.at[o - 1, q - 1, u], wy_r.at[o - 1, q - 1, u], {"grp": lax.rem(y + q, g)}
        )

    def w_c(o, q, u):
        ref = wfull.at[xs(o), w_rows(lax.rem(y + g - q, g), u)]
        return remote(ref, ref, wc_s.at[o - 1, q, u], wc_r.at[o - 1, q, u], partner)

    w_own = remote(w_ref, wfull.at[dp], wo_s, wo_r, partner)

    items = []
    for u in range(units):
        if u * m % units < m:
            items.append(("k", u * m // units))
        items.append(("w", u))

    def issue(s):
        if s >= len(items):
            return
        kind, e = items[s]
        if kind == "k":
            if e > 0:
                kz_copy(m - e).wait_recv()
            for o in range(1, nx):
                k_x(o, e).start()
            k_own(e).start()
        else:
            for o in range(1, nx):
                w_x(o, e).start()

    def pass_x(s):
        if s >= len(items):
            return
        kind, e = items[s]
        in_x, in_y, in_c = (k_x, k_y, k_c) if kind == "k" else (w_x, w_y, w_c)
        for o in range(1, nx):
            in_x(o, e).wait_recv()
            for q in range(1, g):
                in_y(o, q, e).start()
            in_c(o, 0, e).start()

    def pass_y(s):
        if s < 0 or s >= len(items):
            return
        kind, e = items[s]
        in_y, in_c = (k_y, k_c) if kind == "k" else (w_y, w_c)
        for o in range(1, nx):
            for q in range(1, g):
                in_y(o, q, e).wait_recv()
                in_c(o, q, e).start()

    done = []

    def step():
        s = len(done)
        done.append(s)
        issue(s + LEAD)
        pass_x(s)
        pass_y(s - LAG)

    for o in range(1, m):
        kz_copy(o).start()
    issue(0)
    for o in range(1, n):
        @pl.when(lat_sent(o))
        def _():
            for copy in lat_copies(o):
                copy.start()
    for e in range(m):
        for s in range(1, p):
            q_copy(s, e).start()
    for s in range(1, LEAD):
        issue(s)
    w_own.start()

    before = len(items) // 2 + 1
    for s in range(before):
        step()

    for o in range(1, n):
        @pl.when(lat_taken(o))
        def _():
            for copy in lat_copies(o):
                copy.wait_recv()

    @pl.loop(0, (b + 1) * p)
    def _(j):
        turn = jnp.concatenate(
            [rkey[j, :, f * tok : (f + 1) * tok] for f in range(rope // rrows)], axis=0
        ).astype(jnp.float32)
        filled = jnp.concatenate([turn, jnp.zeros((LANES - rope, tok), jnp.float32)], axis=0)
        shared[span(j * tok, tok), :] = filled.T.astype(jnp.bfloat16)

    variants = math.gcd(VARIANTS, m)
    stride = length // variants
    if stride > p * tok:
        @pl.loop((b + 1) * p, n)
        def _(j):
            rows = span(j * tok, tok)
            lat[rows, :] = jnp.zeros((tok, latw), lat.dtype)
            shared[rows, :] = jnp.zeros((tok, LANES), shared.dtype)

    def head_over(i, h, extent):
        row = lax.broadcasted_iota(jnp.int32, (stride, p * tok), 0)
        col = lax.broadcasted_iota(jnp.int32, (stride, p * tok), 1)
        kept = row - col <= b * (p * tok) - (extent - stride)
        both = jnp.dot(
            lat[:extent, :], kvw[i, :, h * wide : (h + 1) * wide], preferred_element_type=jnp.float32
        )
        keys = jnp.concatenate([both[:, :NOPE].astype(jnp.bfloat16), shared[:extent, :]], axis=1)
        values = both[:, NOPE:].T.astype(jnp.bfloat16)
        raw = jnp.concatenate([qbuf[t, i, h, :, :] for t in range(p)], axis=1)
        first, second = turned(raw[NOPE:], table[0], table[1])
        query = jnp.concatenate(
            [
                raw[:NOPE], first.astype(jnp.bfloat16), second.astype(jnp.bfloat16),
                jnp.zeros((LANES - rope, p * tok), jnp.bfloat16),
            ],
            axis=0,
        )
        s = jnp.dot(keys, query, preferred_element_type=jnp.float32)
        last = jnp.where(kept, s[extent - stride :], -jnp.inf)
        s = last if extent == stride else jnp.concatenate([s[: extent - stride], last], axis=0)
        top = jnp.max(s, axis=0, keepdims=True)
        e = jnp.exp2((s - top) * (scale * math.log2(math.e)))
        probs = (e * (1.0 / jnp.sum(e, axis=0, keepdims=True))).astype(jnp.bfloat16)
        o = jnp.dot(values, probs, preferred_element_type=jnp.float32)
        for t in range(p):
            attout[i, t, h] = o[:, t * tok : (t + 1) * tok].T.astype(jnp.bfloat16)

    def head(i, h):
        for v in range(variants):
            @pl.when(lax.div(b, m // variants) == v)
            def _():
                head_over(i, h, (v + 1) * stride)

    def take_q(e):
        i = group(e)
        own_q(i).wait()
        for s in range(1, p):
            q_copy(s, e).wait_recv()

    def take_k(e):
        k_own(e).wait_recv()
        for o in range(1, nx):
            for q in range(g):
                k_c(o, q, e).wait_recv()

    own_k.wait()
    if m * hn <= 2 * VARIANTS:
        for e in range(m):
            if e > 0:
                while len(done) <= items.index(("k", e)) + LAG:
                    step()
            take_q(e)
            take_k(e)
            for h in range(hn):
                head(group(e), h)
                for s in range(1, p):
                    a_copy(s, group(e), h).start()
                step()
        while len(done) < len(items) + LAG:
            step()
    else:
        while len(done) < len(items) + LAG:
            step()
        for e in range(m):
            take_q(e)
            take_k(e)

        @pl.loop(0, m)
        def _(e):
            i = lax.rem(b + e, m)
            for h in range(hn):
                head(i, h)
                for s in range(1, p):
                    a_copy(s, i, h).start()

    own_w.wait()
    w_own.wait_recv()

    for k in range(n):
        for u in range(k * sub, (k + 1) * sub):
            for o in range(1, nx):
                for q in range(g):
                    w_c(o, q, u).wait_recv()
        q, i = place(k)
        if k % p == 0:
            block = jnp.concatenate([attout[i, r, h] for h in range(hn)], axis=1)
        else:
            for h in range(hn):
                a_copy(p - k % p, i, h).wait_recv()
            block = jnp.concatenate([attin[q, i, h] for h in range(hn)], axis=1)
        rows = span((q + p * i) * kd, kd)
        for d in range(ndp):
            part_sum = jnp.dot(block, wfull[d, rows, :], preferred_element_type=jnp.float32)
            where = slice(d * cols, (d + 1) * cols)
            if k == 0:
                acc[:, where] = part_sum
            elif k < n - 1:
                acc[:, where] += part_sum
            else:
                out_ref[:, where] = (acc[:, where] + part_sum).astype(out_ref.dtype)

    for o in range(1, n):
        @pl.when(lat_sent(o))
        def _():
            for copy in lat_copies(o):
                copy.wait_send()
    for o in range(1, m):
        kz_copy(o).wait_send()
    for e in range(m):
        k_own(e).wait_send()
        for s in range(1, p):
            q_copy(s, e).wait_send()
            for h in range(hn):
                a_copy(s, group(e), h).wait_send()
    w_own.wait_send()
    for kind, e in items:
        in_x, in_y, in_c = (k_x, k_y, k_c) if kind == "k" else (w_x, w_y, w_c)
        for o in range(1, nx):
            in_x(o, e).wait_send()
            for q in range(1, g):
                in_y(o, q, e).wait_send()
            for q in range(g):
                in_c(o, q, e).wait_send()


def body(sizes, queries, kv_latent, rope_key, kv_gain, kv_weight, out_weight):
    g, n, dp = sizes
    nx = dp // CORES
    tok, heads, width = queries.shape[1:]
    rope = width - NOPE
    hn = heads // n
    latw = kv_latent.shape[2]
    p = math.gcd(SPLIT, n)
    m = n // p
    sub = max(1, UNITS // n)
    units = n * sub
    q = jnp.transpose(queries[0], (1, 2, 0))
    key = jnp.transpose(rope_key[0])
    table = jnp.asarray(rotation_table(n * tok, rope))

    d_in, cols = out_weight.shape
    kcols = kv_weight.shape[1]
    dma = pltpu.SemaphoreType.DMA
    bf = jnp.bfloat16
    xn = max(nx - 1, 1)
    gn = max(g - 1, 1)
    pn = max(p - 1, 1)
    mn = max(m - 1, 1)
    vmem = pl.BlockSpec(memory_space=pltpu.VMEM)
    hbm = pl.BlockSpec(memory_space=pltpu.HBM)
    out = pl.pallas_call(
        functools.partial(kernel, n, g, nx, p, hn, rope, width**-0.5, sub),
        out_shape=jax.ShapeDtypeStruct((tok, cols * dp), bf),
        in_specs=[hbm] * 7,
        out_specs=vmem,
        scratch_shapes=[
            pltpu.VMEM((p, m, hn, width, tok), bf),
            pltpu.VMEM((n * tok, latw), bf),
            pltpu.VMEM((n, rope * tok // latw, latw), bf),
            pltpu.VMEM((n * tok, LANES), bf),
            pltpu.VMEM((m, kv_weight.shape[0] * dp, kcols), bf),
            pltpu.VMEM((dp, d_in, cols), bf),
            pltpu.VMEM((m, p, hn, tok, VD), bf),
            pltpu.VMEM((p, m, hn, tok, VD), bf),
            pltpu.VMEM((tok, cols * dp), jnp.float32),
            pltpu.VMEM((tok, latw), bf),
            pltpu.VMEM((rope, tok), bf),
            pltpu.VMEM((1, latw), jnp.float32),
            pltpu.VMEM((2, rope // 2, p * tok), jnp.float32),
            dma((6 + m,)),
            dma((n,)), dma((n,)), dma((n,)), dma((n,)),
            dma((pn, m)), dma((pn, m)),
            dma((mn,)), dma((mn,)),
            dma((pn, m, hn)), dma((pn, m, hn)),
            dma((xn, m)), dma((xn, m)),
            dma((xn, gn, m)), dma((xn, gn, m)),
            dma((xn, g, m)), dma((xn, g, m)),
            dma((m,)), dma((m,)),
            dma((xn, units)), dma((xn, units)),
            dma((xn, gn, units)), dma((xn, gn, units)),
            dma((xn, g, units)), dma((xn, g, units)),
            dma(()), dma(()),
        ],
        compiler_params=pltpu.CompilerParams(
            collective_id=0, has_side_effects=True, vmem_limit_bytes=60 * 1024 * 1024
        ),
    )(q, kv_latent[0], key, kv_gain[None], table, kv_weight, out_weight)
    return out[None]


def solution(mesh):
    sizes = (mesh.shape["grp"], mesh.shape["sp"], mesh.shape["dp"])
    return jax.shard_map(
        functools.partial(body, sizes),
        mesh=mesh,
        in_specs=(
            P(("grp", "dp"), "sp", None, None),
            P(("grp", "dp"), "sp", None),
            P(("grp", "dp"), "sp", None),
            P(),
            P("dp", "sp"),
            P(None, "dp"),
        ),
        out_specs=P(("grp", "dp"), "sp", None),
        check_vma=False,
    )
```

```python
import functools
import math

import jax
import jax.numpy as jnp
import numpy as np
from jax import lax
from jax.experimental import pallas as pl
from jax.experimental.pallas import tpu as pltpu
from jax.sharding import PartitionSpec as P

NOPE = 128
VD = 128
LANES = 128
CORES = 2
UNITS = 16
LEAD = 4
LAG = 4
KEYS = 7
RELAY = 8
LATE = 12
START = 12
DIRECT = 1
PLAN = (1, 1, 1, 1, 2, 2, 1, 1, 1)
SPLIT = 2
VARIANTS = 4
MESH = pl.DeviceIdType.MESH


def rotation_table(length, rope):
    half = rope // 2
    inverse = np.power(10000.0, -np.arange(half) * 2.0 / rope).astype(np.float32)
    angle = inverse[:, None] * np.arange(length, dtype=np.float32)[None, :]
    return np.stack([np.cos(angle), np.sin(angle)]).astype(np.float32)


def kernel(
    n, g, nx, p, hn, rope, scale, sub,
    q_ref, latent_ref, key_ref, gain_ref, table_ref, kvw_ref, w_ref, out_ref,
    qbuf, lat, rkey, shared, kvw, wfull, attout, attin, acc, latin, keyin, gain, table,
    loc, lm_s, lm_r, lg_s, lg_r, lr_s, lr_r, q_s, q_r, kz_s, kz_r, a_s, a_r,
    kx_s, kx_r, ky_s, ky_r, kc_s, kc_r, ko_s, ko_r,
    wx_s, wx_r, wy_s, wy_r, wc_s, wc_r, wo_s, wo_r, far,
):
    me = lax.axis_index("sp")
    y = lax.axis_index("grp")
    dp = lax.axis_index("dp")
    x, c = dp // CORES, dp % CORES
    b, r = lax.div(me, p), lax.rem(me, p)
    m = n // p
    ndp = nx * CORES
    tok, latw = latent_ref.shape
    half = rope // 2
    rrows = rkey.shape[1]
    krows = kvw_ref.shape[0]
    kh = krows // g
    cols = w_ref.shape[1]
    kd = hn * VD
    part = kd // g
    crow = part // sub
    units = n * sub
    length = n * tok
    wide = NOPE + VD

    def chip(xx, cc):
        return {"dp": xx * CORES + cc}

    partner = chip(x, 1 - c)

    def remote(src, dst, ss, rs, dev):
        return pltpu.make_async_remote_copy(
            src_ref=src, dst_ref=dst, send_sem=ss, recv_sem=rs, device_id=dev, device_id_type=MESH
        )

    def span(start, size):
        return pl.ds(pl.multiple_of(start, size), size)

    def mate(s):
        return lax.rem(r + s, p)

    def group(o):
        return lax.rem(b + o, m)

    def xs(o):
        return lax.rem(x + nx - o, nx) * CORES + c

    get_lat = pltpu.make_async_copy(latent_ref, latin, loc.at[0])
    get_key = pltpu.make_async_copy(key_ref, keyin, loc.at[1])
    get_gain = pltpu.make_async_copy(gain_ref, gain, loc.at[2])
    get_table = pltpu.make_async_copy(table_ref.at[:, :, span(b * (p * tok), p * tok)], table, loc.at[3])
    own_k = pltpu.make_async_copy(kvw_ref, kvw.at[b, span(dp * krows, krows)], loc.at[4])
    own_w = pltpu.make_async_copy(w_ref, wfull.at[dp], loc.at[5])

    def own_q(i):
        return pltpu.make_async_copy(q_ref.at[span((r + p * i) * hn, hn)], qbuf.at[r, i], loc.at[6 + i])

    for copy in (get_lat, get_key, get_gain, get_table):
        copy.start()

    barrier = pltpu.get_barrier_semaphore()
    staged = (m - 1) * p == 2

    def greet(semaphore):
        @pl.when(me > 0)
        def _():
            pl.semaphore_signal(semaphore, 1, device_id={"sp": me - 1}, device_id_type=MESH)

        @pl.when(me < n - 1)
        def _():
            pl.semaphore_signal(semaphore, 1, device_id={"sp": me + 1}, device_id_type=MESH)

    beside = jnp.where(me > 0, 1, 0) + jnp.where(me < n - 1, 1, 0)
    if staged:
        greet(barrier)
    else:
        for s in range(1, p):
            pl.semaphore_signal(barrier, 1, device_id={"sp": b * p + mate(s)}, device_id_type=MESH)
        for o in range(1, m):
            pl.semaphore_signal(barrier, 1, device_id={"sp": group(o) * p + r}, device_id_type=MESH)
    for o in range(1, nx):
        pl.semaphore_signal(barrier, 1, device_id=chip(lax.rem(x + o, nx), c), device_id_type=MESH)
    for o in range(1, g):
        pl.semaphore_signal(barrier, 1, device_id={"grp": lax.rem(y + o, g)}, device_id_type=MESH)
    pl.semaphore_signal(barrier, 1, device_id=partner, device_id_type=MESH)

    own_k.start()
    for i in range(m):
        own_q(i).start()
    own_w.start()

    def turned(values, cosine, sine):
        first, second = values[:half].astype(jnp.float32), values[half:].astype(jnp.float32)
        return first * cosine - second * sine, first * sine + second * cosine

    def kz_copy(o, q):
        part_of = lax.rem(y + q, g)
        return remote(
            kvw_ref.at[span(part_of * kh, kh)], k_rows(b, dp, part_of),
            kz_s.at[o - 1, q], kz_r.at[o - 1, q], {"sp": group(o) * p + r},
        )

    def lat_pair(j, to, ss, rs):
        rows = span(j * tok, tok)
        return (
            remote(lat.at[rows], lat.at[rows], ss.at[0], rs.at[0], {"sp": to}),
            remote(rkey.at[j], rkey.at[j], ss.at[1], rs.at[1], {"sp": to}),
        )

    def lat_mate(s):
        return lat_pair(me, b * p + mate(s), lm_s.at[s - 1], lm_r.at[s - 1])

    def lat_group(o):
        return lat_pair(me, group(o) * p + r, lg_s.at[o - 1], lg_r.at[o - 1])

    def lat_relay(o, s):
        j = lax.rem(b + m - o, m) * p + r
        return lat_pair(j, b * p + mate(s), lr_s.at[o - 1, s - 1], lr_r.at[o - 1, s - 1])

    def relay():
        for o in range(1, m):
            @pl.when(b - o >= 0)
            def _():
                for copy in lat_group(o):
                    copy.wait_recv()
                for s in range(1, p):
                    for copy in lat_relay(o, s):
                        copy.start()

    def q_copy(s, e):
        t, i = mate(s), group(e)
        return remote(
            q_ref.at[span((t + p * i) * hn, hn)], qbuf.at[r, i], q_s.at[s - 1, i], q_r.at[s - 1, i],
            {"sp": b * p + t},
        )

    def a_copy(s, i, h):
        t = mate(s)
        return remote(
            attout.at[i, t, h], attin.at[r, i, h], a_s.at[s - 1, i, h], a_r.at[s - 1, i, h],
            {"sp": b * p + t},
        )

    def k_rows(i, d, q):
        return kvw.at[i, span(d * krows + q * kh, kh)]

    def k_x(o, e):
        dst = k_rows(group(e), dp, y)
        src = kvw_ref.at[span(y * kh, kh)] if e == 0 else dst
        return remote(
            src, dst, kx_s.at[o - 1, e], kx_r.at[o - 1, e], chip(lax.rem(x + o, nx), c)
        )

    def k_y(o, q, e):
        ref = k_rows(group(e), xs(o), y)
        return remote(
            ref, ref, ky_s.at[o - 1, q - 1, e], ky_r.at[o - 1, q - 1, e], {"grp": lax.rem(y + q, g)}
        )

    def k_c(o, q, e):
        ref = k_rows(group(e), xs(o), lax.rem(y + g - q, g))
        return remote(ref, ref, kc_s.at[o - 1, q, e], kc_r.at[o - 1, q, e], partner)

    def k_own(q, e):
        part_of = lax.rem(y + q, g)
        dst = k_rows(group(e), dp, part_of)
        src = kvw_ref.at[span(part_of * kh, kh)] if e == 0 else dst
        return remote(src, dst, ko_s.at[q, e], ko_r.at[q, e], partner)

    def late():
        for e in range(1, m):
            for q in range(1, g):
                kz_copy(m - e, q).wait_recv()
                k_own(q, e).start()

    def place(k):
        return lax.rem(r + k % p, p), group(k // p)

    def w_rows(yy, u):
        q, i = place(u // sub)
        return span((q + p * i) * kd + yy * part + (u % sub) * crow, crow)

    def direct(kind, u):
        return kind == "w" and u >= units - DIRECT

    def w_x(o, u, q=0):
        rows = w_rows(lax.rem(y + g - q, g), u)
        sems = (wx_s.at[o - 1, u], wx_r.at[o - 1, u])
        if q > 0:
            sems = (wy_s.at[o - 1, q - 1, u], wy_r.at[o - 1, q - 1, u])
        return remote(w_ref.at[rows], wfull.at[dp, rows], *sems, chip(lax.rem(x + o, nx), c))

    def w_y(o, q, u):
        ref = wfull.at[xs(o), w_rows(y, u)]
        return remote(
            ref, ref, wy_s.at[o - 1, q - 1, u], wy_r.at[o - 1, q - 1, u], {"grp": lax.rem(y + q, g)}
        )

    def w_c(o, q, u):
        ref = wfull.at[xs(o), w_rows(lax.rem(y + g - q, g), u)]
        return remote(ref, ref, wc_s.at[o - 1, q, u], wc_r.at[o - 1, q, u], partner)

    w_own = remote(w_ref, wfull.at[dp], wo_s, wo_r, partner)

    items = [("w", u) for u in range(units)]
    for e in range(1, m):
        items.insert(KEYS + (e - 1) * (units - KEYS) // (m - 1), ("k", e))
    items.insert(1, ("k", 0))

    def issue(s):
        if s >= len(items):
            return
        kind, e = items[s]
        if kind == "k":
            if e > 0:
                kz_copy(m - e, 0).wait_recv()
            for o in range(1, nx):
                k_x(o, e).start()
            for q in range(g if e == 0 else 1):
                k_own(q, e).start()
        else:
            for o in range(1, nx):
                for q in range(g if direct(kind, e) else 1):
                    w_x(o, e, q).start()

    def pass_x(s):
        if s >= len(items):
            return
        kind, e = items[s]
        for o in range(1, nx):
            if direct(kind, e):
                for q in range(g):
                    w_x(o, e, q).wait_recv()
                    w_c(o, q, e).start()
                continue
            in_x, in_y, in_c = (k_x, k_y, k_c) if kind == "k" else (w_x, w_y, w_c)
            in_x(o, e).wait_recv()
            for q in range(1, g):
                in_y(o, q, e).start()
            in_c(o, 0, e).start()

    def pass_y(s):
        if s < 0 or s >= len(items) or direct(*items[s]):
            return
        kind, e = items[s]
        in_y, in_c = (k_y, k_c) if kind == "k" else (w_y, w_c)
        for o in range(1, nx):
            for q in range(1, g):
                in_y(o, q, e).wait_recv()
                in_c(o, q, e).start()

    done = []

    def step():
        s = len(done)
        if s >= len(items) + LAG:
            return
        done.append(s)
        if s == RELAY:
            relay()
            for e in range(1, m):
                for o in range(1, p):
                    q_copy(o, e).start()
        if s == LATE:
            late()
        issue(s + LEAD)
        pass_x(s)
        pass_y(s - LAG)

    along = beside if staged else (p - 1) + (m - 1)
    pl.semaphore_wait(barrier, along + (nx - 1) + (g - 1) + 1)
    if staged:
        greet(far)
    for s in range(LEAD):
        issue(s)

    get_lat.wait()
    get_gain.wait()
    latent = latin[...].astype(jnp.float32)
    square = jnp.mean(latent * latent, axis=-1, keepdims=True)
    lat[span(me * tok, tok), :] = (latent * lax.rsqrt(square + 1e-06) * gain[...]).astype(jnp.bfloat16)
    get_key.wait()
    get_table.wait()
    mine = span(r * tok, tok)
    first, second = turned(keyin[...], table[0, :, mine], table[1, :, mine])
    both = jnp.concatenate([first, second], axis=0).astype(jnp.bfloat16)
    for f in range(rope // rrows):
        rkey[me, :, f * tok : (f + 1) * tok] = both[f * rrows : (f + 1) * rrows]

    if staged:
        pl.semaphore_wait(far, beside)
    for o in range(1, m):
        kz_copy(o, 0).start()
    for o in range(1, m):
        @pl.when(b + o < m)
        def _():
            for copy in lat_group(o):
                copy.start()
    for s in range(1, p):
        for copy in lat_mate(s):
            copy.start()
    for o in range(1, m):
        for q in range(1, g):
            kz_copy(o, q).start()
    for s in range(1, p):
        q_copy(s, 0).start()
    w_own.start()

    for s in range(START):
        step()

    for s in range(1, p):
        for copy in lat_mate(s):
            copy.wait_recv()
    for o in range(1, m):
        @pl.when(b - o >= 0)
        def _():
            for s in range(1, p):
                for copy in lat_relay(o, s):
                    copy.wait_recv()

    @pl.loop(0, (b + 1) * p)
    def _(j):
        turn = jnp.concatenate(
            [rkey[j, :, f * tok : (f + 1) * tok] for f in range(rope // rrows)], axis=0
        ).astype(jnp.float32)
        filled = jnp.concatenate([turn, jnp.zeros((LANES - rope, tok), jnp.float32)], axis=0)
        shared[span(j * tok, tok), :] = filled.T.astype(jnp.bfloat16)

    variants = math.gcd(VARIANTS, m)
    stride = length // variants
    if stride > p * tok:
        @pl.loop((b + 1) * p, n)
        def _(j):
            rows = span(j * tok, tok)
            lat[rows, :] = jnp.zeros((tok, latw), lat.dtype)
            shared[rows, :] = jnp.zeros((tok, LANES), shared.dtype)

    def head_over(i, h, extent):
        row = lax.broadcasted_iota(jnp.int32, (stride, p * tok), 0)
        col = lax.broadcasted_iota(jnp.int32, (stride, p * tok), 1)
        kept = row - col <= b * (p * tok) - (extent - stride)
        both = jnp.dot(
            lat[:extent, :], kvw[i, :, h * wide : (h + 1) * wide], preferred_element_type=jnp.float32
        )
        keys = jnp.concatenate([both[:, :NOPE].astype(jnp.bfloat16), shared[:extent, :]], axis=1)
        values = both[:, NOPE:].T.astype(jnp.bfloat16)
        raw = jnp.concatenate([qbuf[t, i, h, :, :] for t in range(p)], axis=1)
        first, second = turned(raw[NOPE:], table[0], table[1])
        query = jnp.concatenate(
            [
                raw[:NOPE], first.astype(jnp.bfloat16), second.astype(jnp.bfloat16),
                jnp.zeros((LANES - rope, p * tok), jnp.bfloat16),
            ],
            axis=0,
        )
        s = jnp.dot(keys, query, preferred_element_type=jnp.float32)
        last = jnp.where(kept, s[extent - stride :], -jnp.inf)
        s = last if extent == stride else jnp.concatenate([s[: extent - stride], last], axis=0)
        top = jnp.max(s, axis=0, keepdims=True)
        e = jnp.exp2((s - top) * (scale * math.log2(math.e)))
        probs = (e * (1.0 / jnp.sum(e, axis=0, keepdims=True))).astype(jnp.bfloat16)
        o = jnp.dot(values, probs, preferred_element_type=jnp.float32)
        for t in range(p):
            attout[i, t, h] = o[:, t * tok : (t + 1) * tok].T.astype(jnp.bfloat16)

    def head(i, h):
        for v in range(variants):
            @pl.when(lax.div(b, m // variants) == v)
            def _():
                head_over(i, h, (v + 1) * stride)

    def take_q(e):
        i = group(e)
        own_q(i).wait()
        for s in range(1, p):
            q_copy(s, e).wait_recv()

    def take_k(e):
        for q in range(g):
            k_own(q, e).wait_recv()
        for o in range(1, nx):
            for q in range(g):
                k_c(o, q, e).wait_recv()

    def attend(e, h):
        if h == 0:
            while e > 0 and len(done) <= items.index(("k", e)) + LAG:
                step()
            take_q(e)
            take_k(e)
        head(group(e), h)
        for s in range(1, p):
            a_copy(s, group(e), h).start()

    def project(k):
        while len(done) < min(len(items), items.index(("w", (k + 1) * sub - 1)) + 1) + LAG:
            step()
        if k == 0:
            own_w.wait()
            w_own.wait_recv()
        for u in range(k * sub, (k + 1) * sub):
            for o in range(1, nx):
                for q in range(g):
                    w_c(o, q, u).wait_recv()
        q, i = place(k)
        if k % p == 0:
            block = jnp.concatenate([attout[i, r, h] for h in range(hn)], axis=1)
        else:
            for h in range(hn):
                a_copy(p - k % p, i, h).wait_recv()
            block = jnp.concatenate([attin[q, i, h] for h in range(hn)], axis=1)
        rows = span((q + p * i) * kd, kd)
        for d in range(ndp):
            part_sum = jnp.dot(block, wfull[d, rows, :], preferred_element_type=jnp.float32)
            where = slice(d * cols, (d + 1) * cols)
            if k == 0:
                acc[:, where] = part_sum
            elif k < n - 1:
                acc[:, where] += part_sum
            else:
                out_ref[:, where] = (acc[:, where] + part_sum).astype(out_ref.dtype)

    own_k.wait()
    work = [functools.partial(project, k) for k in range(n)]
    if m * hn <= 2 * VARIANTS:
        work = [functools.partial(attend, e, h) for e in range(m) for h in range(hn)] + work
    else:
        while len(done) < len(items) + LAG:
            step()
        for e in range(m):
            take_q(e)
            take_k(e)

        @pl.loop(0, m)
        def _(e):
            i = lax.rem(b + e, m)
            for h in range(hn):
                head(i, h)
                for s in range(1, p):
                    a_copy(s, i, h).start()

    for count in PLAN:
        for _ in range(min(count, len(work))):
            work.pop(0)()
        step()
    for piece in work:
        piece()
    while len(done) < len(items) + LAG:
        step()

    for s in range(1, p):
        for copy in lat_mate(s):
            copy.wait_send()
    for o in range(1, m):
        @pl.when(b + o < m)
        def _():
            for copy in lat_group(o):
                copy.wait_send()

        @pl.when(b - o >= 0)
        def _():
            for s in range(1, p):
                for copy in lat_relay(o, s):
                    copy.wait_send()
    for o in range(1, m):
        for q in range(g):
            kz_copy(o, q).wait_send()
    for e in range(m):
        for q in range(g):
            k_own(q, e).wait_send()
        for s in range(1, p):
            q_copy(s, e).wait_send()
            for h in range(hn):
                a_copy(s, group(e), h).wait_send()
    w_own.wait_send()
    for kind, e in items:
        in_x, in_y, in_c = (k_x, k_y, k_c) if kind == "k" else (w_x, w_y, w_c)
        for o in range(1, nx):
            in_x(o, e).wait_send()
            for q in range(1, g):
                if direct(kind, e):
                    w_x(o, e, q).wait_send()
                else:
                    in_y(o, q, e).wait_send()
            for q in range(g):
                in_c(o, q, e).wait_send()


def body(sizes, queries, kv_latent, rope_key, kv_gain, kv_weight, out_weight):
    g, n, dp = sizes
    nx = dp // CORES
    tok, heads, width = queries.shape[1:]
    rope = width - NOPE
    hn = heads // n
    latw = kv_latent.shape[2]
    p = math.gcd(SPLIT, n)
    m = n // p
    sub = max(1, UNITS // n)
    units = n * sub
    q = jnp.transpose(queries[0], (1, 2, 0))
    key = jnp.transpose(rope_key[0])
    table = jnp.asarray(rotation_table(n * tok, rope))

    d_in, cols = out_weight.shape
    kcols = kv_weight.shape[1]
    dma = pltpu.SemaphoreType.DMA
    bf = jnp.bfloat16
    xn = max(nx - 1, 1)
    gn = max(g - 1, 1)
    pn = max(p - 1, 1)
    mn = max(m - 1, 1)
    vmem = pl.BlockSpec(memory_space=pltpu.VMEM)
    hbm = pl.BlockSpec(memory_space=pltpu.HBM)
    out = pl.pallas_call(
        functools.partial(kernel, n, g, nx, p, hn, rope, width**-0.5, sub),
        out_shape=pltpu.VMEM((tok, cols * dp), bf),
        in_specs=[hbm] * 7,
        out_specs=vmem,
        scratch_shapes=[
            pltpu.VMEM((p, m, hn, width, tok), bf),
            pltpu.VMEM((n * tok, latw), bf),
            pltpu.VMEM((n, rope * tok // latw, latw), bf),
            pltpu.VMEM((n * tok, LANES), bf),
            pltpu.VMEM((m, kv_weight.shape[0] * dp, kcols), bf),
            pltpu.VMEM((dp, d_in, cols), bf),
            pltpu.VMEM((m, p, hn, tok, VD), bf),
            pltpu.VMEM((p, m, hn, tok, VD), bf),
            pltpu.VMEM((tok, cols * dp), jnp.float32),
            pltpu.VMEM((tok, latw), bf),
            pltpu.VMEM((rope, tok), bf),
            pltpu.VMEM((1, latw), jnp.float32),
            pltpu.VMEM((2, rope // 2, p * tok), jnp.float32),
            dma((6 + m,)),
            dma((pn, 2)), dma((pn, 2)), dma((mn, 2)), dma((mn, 2)),
            dma((mn, pn, 2)), dma((mn, pn, 2)),
            dma((pn, m)), dma((pn, m)),
            dma((mn, g)), dma((mn, g)),
            dma((pn, m, hn)), dma((pn, m, hn)),
            dma((xn, m)), dma((xn, m)),
            dma((xn, gn, m)), dma((xn, gn, m)),
            dma((xn, g, m)), dma((xn, g, m)),
            dma((g, m)), dma((g, m)),
            dma((xn, units)), dma((xn, units)),
            dma((xn, gn, units)), dma((xn, gn, units)),
            dma((xn, g, units)), dma((xn, g, units)),
            dma(()), dma(()),
            pltpu.SemaphoreType.REGULAR,
        ],
        compiler_params=pltpu.CompilerParams(
            collective_id=0, has_side_effects=True, vmem_limit_bytes=60 * 1024 * 1024
        ),
    )(q, kv_latent[0], key, kv_gain[None], table, kv_weight, out_weight)
    return out[None]


def solution(mesh):
    sizes = (mesh.shape["grp"], mesh.shape["sp"], mesh.shape["dp"])
    return jax.shard_map(
        functools.partial(body, sizes),
        mesh=mesh,
        in_specs=(
            P(("grp", "dp"), "sp", None, None),
            P(("grp", "dp"), "sp", None),
            P(("grp", "dp"), "sp", None),
            P(),
            P("dp", "sp"),
            P(None, "dp"),
        ),
        out_specs=P(("grp", "dp"), "sp", None),
        check_vma=False,
    )
```

```python
import functools
import math

import jax
import jax.numpy as jnp
import numpy as np
from jax import lax
from jax.experimental import pallas as pl
from jax.experimental.pallas import tpu as pltpu
from jax.sharding import PartitionSpec as P

NOPE = 128
VD = 128
LANES = 128
CORES = 2
UNITS = 16
LEAD = 4
LAG = 4
KEYS = 8
RELAY = 9
LATE = 13
START = 14
DIRECT = 1
PIECES = 2
TILE = 16
APART = 1
EXTRA = 1
HEADS = 2
KEEP = 7
PLAN = (1, 0, 1, 0, 1, 1, 1, 1, 1)
SPLIT = 2
VARIANTS = 4
MESH = pl.DeviceIdType.MESH


def rotation_table(length, rope):
    half = rope // 2
    inverse = np.power(10000.0, -np.arange(half) * 2.0 / rope).astype(np.float32)
    angle = inverse[:, None] * np.arange(length, dtype=np.float32)[None, :]
    return np.stack([np.cos(angle), np.sin(angle)]).astype(np.float32)


def kernel(
    n, g, nx, p, hn, rope, scale, sub,
    q_ref, latent_ref, key_ref, gain_ref, table_ref, kvw_ref, w_ref, out_ref,
    qbuf, lat, rkey, shared, kvw, wfull, attout, attin, acc, latin, keyin, gain, table,
    loc, lm_s, lm_r, lg_s, lg_r, lr_s, lr_r, q_s, q_r, kz_s, kz_r, a_s, a_r,
    kx_s, kx_r, kf_s, kf_r, ky_s, ky_r, kc_s, kc_r, ko_s, ko_r,
    wx_s, wx_r, wy_s, wy_r, wc_s, wc_r, wo_s, wo_r, far,
):
    me = lax.axis_index("sp")
    y = lax.axis_index("grp")
    dp = lax.axis_index("dp")
    x, c = dp // CORES, dp % CORES
    b, r = lax.div(me, p), lax.rem(me, p)
    m = n // p
    ndp = nx * CORES
    tok, latw = latent_ref.shape
    half = rope // 2
    rrows = rkey.shape[1]
    krows = kvw_ref.shape[0]
    kh = krows // g
    pieces = math.gcd(PIECES, max(1, kh // TILE))
    ks = kh // pieces
    cols = w_ref.shape[1]
    kd = hn * VD
    part = kd // g
    crow = part // sub
    units = n * sub
    length = n * tok
    wide = NOPE + VD

    def chip(xx, cc):
        return {"dp": xx * CORES + cc}

    partner = chip(x, 1 - c)

    def remote(src, dst, ss, rs, dev):
        return pltpu.make_async_remote_copy(
            src_ref=src, dst_ref=dst, send_sem=ss, recv_sem=rs, device_id=dev, device_id_type=MESH
        )

    def span(start, size):
        return pl.ds(pl.multiple_of(start, size), size)

    def mate(s):
        return lax.rem(r + s, p)

    def group(o):
        return lax.rem(b + o, m)

    def xs(o):
        return lax.rem(x + nx - o, nx) * CORES + c

    get_lat = pltpu.make_async_copy(latent_ref, latin, loc.at[0])
    get_key = pltpu.make_async_copy(key_ref, keyin, loc.at[1])
    get_gain = pltpu.make_async_copy(gain_ref, gain, loc.at[2])
    get_table = pltpu.make_async_copy(table_ref.at[:, :, span(b * (p * tok), p * tok)], table, loc.at[3])
    own_k = pltpu.make_async_copy(kvw_ref, kvw.at[b, span(dp * krows, krows)], loc.at[4])
    own_w = pltpu.make_async_copy(w_ref, wfull.at[dp], loc.at[5])

    def own_q(i):
        return pltpu.make_async_copy(q_ref.at[span((r + p * i) * hn, hn)], qbuf.at[r, i], loc.at[6 + i])

    for copy in (get_lat, get_key, get_gain, get_table):
        copy.start()

    barrier = pltpu.get_barrier_semaphore()
    staged = (m - 1) * p == 2

    def greet(semaphore):
        @pl.when(me > 0)
        def _():
            pl.semaphore_signal(semaphore, 1, device_id={"sp": me - 1}, device_id_type=MESH)

        @pl.when(me < n - 1)
        def _():
            pl.semaphore_signal(semaphore, 1, device_id={"sp": me + 1}, device_id_type=MESH)

    beside = jnp.where(me > 0, 1, 0) + jnp.where(me < n - 1, 1, 0)
    if staged:
        greet(barrier)
    else:
        for s in range(1, p):
            pl.semaphore_signal(barrier, 1, device_id={"sp": b * p + mate(s)}, device_id_type=MESH)
        for o in range(1, m):
            pl.semaphore_signal(barrier, 1, device_id={"sp": group(o) * p + r}, device_id_type=MESH)
    for o in range(1, nx):
        pl.semaphore_signal(barrier, 1, device_id=chip(lax.rem(x + o, nx), c), device_id_type=MESH)
    for o in range(1, g):
        pl.semaphore_signal(barrier, 1, device_id={"grp": lax.rem(y + o, g)}, device_id_type=MESH)
    pl.semaphore_signal(barrier, 1, device_id=partner, device_id_type=MESH)

    own_k.start()
    for i in range(m):
        own_q(i).start()
    own_w.start()

    def turned(values, cosine, sine):
        first, second = values[:half].astype(jnp.float32), values[half:].astype(jnp.float32)
        return first * cosine - second * sine, first * sine + second * cosine

    def kz_copy(o, q):
        part_of = lax.rem(y + q, g)
        return remote(
            kvw_ref.at[span(part_of * kh, kh)], k_rows(b, dp, part_of),
            kz_s.at[o - 1, q], kz_r.at[o - 1, q], {"sp": group(o) * p + r},
        )

    def lat_pair(j, to, ss, rs):
        rows = span(j * tok, tok)
        return (
            remote(lat.at[rows], lat.at[rows], ss.at[0], rs.at[0], {"sp": to}),
            remote(rkey.at[j], rkey.at[j], ss.at[1], rs.at[1], {"sp": to}),
        )

    def lat_mate(s):
        return lat_pair(me, b * p + mate(s), lm_s.at[s - 1], lm_r.at[s - 1])

    def lat_group(o):
        return lat_pair(me, group(o) * p + r, lg_s.at[o - 1], lg_r.at[o - 1])

    def lat_relay(o, s):
        j = lax.rem(b + m - o, m) * p + r
        return lat_pair(j, b * p + mate(s), lr_s.at[o - 1, s - 1], lr_r.at[o - 1, s - 1])

    def relay():
        for o in range(1, m):
            @pl.when(b - o >= 0)
            def _():
                for copy in lat_group(o):
                    copy.wait_recv()
                for s in range(1, p):
                    for copy in lat_relay(o, s):
                        copy.start()

    def q_copy(s, e):
        t, i = mate(s), group(e)
        return remote(
            q_ref.at[span((t + p * i) * hn, hn)], qbuf.at[r, i], q_s.at[s - 1, i], q_r.at[s - 1, i],
            {"sp": b * p + t},
        )

    def a_copy(s, i, h):
        t = mate(s)
        return remote(
            attout.at[i, t, h], attin.at[r, i, h], a_s.at[s - 1, i, h], a_r.at[s - 1, i, h],
            {"sp": b * p + t},
        )

    def k_rows(i, d, q):
        return kvw.at[i, span(d * krows + q * kh, kh)]

    def k_piece(i, d, q, f):
        return kvw.at[i, pl.ds(pl.multiple_of(d * krows + q * kh + f * ks, TILE), ks)]

    def k_x(o, ef):
        e, f = ef
        dst = k_piece(group(e), dp, y, f)
        src = kvw_ref.at[pl.ds(pl.multiple_of(y * kh + f * ks, TILE), ks)] if e == 0 else dst
        return remote(
            src, dst, kx_s.at[o - 1, e, f], kx_r.at[o - 1, e, f], chip(lax.rem(x + o, nx), c)
        )

    def k_down(s, o, f):
        ref = k_piece(b, xs(o), y, f)
        return remote(
            ref, ref, kf_s.at[s - 1, o - 1, f], kf_r.at[s - 1, o - 1, f],
            {"sp": lax.rem(b + m - s, m) * p + r},
        )

    def k_y(o, q, ef):
        e, f = ef
        ref = k_piece(group(e), xs(o), y, f)
        return remote(
            ref, ref, ky_s.at[o - 1, q - 1, e, f], ky_r.at[o - 1, q - 1, e, f],
            {"grp": lax.rem(y + q, g)},
        )

    def k_c(o, q, ef):
        e, f = ef
        ref = k_piece(group(e), xs(o), lax.rem(y + g - q, g), f)
        return remote(ref, ref, kc_s.at[o - 1, q, e, f], kc_r.at[o - 1, q, e, f], partner)

    def k_own(q, e):
        part_of = lax.rem(y + q, g)
        dst = k_rows(group(e), dp, part_of)
        src = kvw_ref.at[span(part_of * kh, kh)] if e == 0 else dst
        return remote(src, dst, ko_s.at[q, e], ko_r.at[q, e], partner)

    def late():
        for e in range(1, m):
            for q in range(1, g):
                kz_copy(m - e, q).wait_recv()
                k_own(q, e).start()

    def place(k):
        return lax.rem(r + k % p, p), group(k // p)

    def w_rows(yy, u):
        q, i = place(u // sub)
        return span((q + p * i) * kd + yy * part + (u % sub) * crow, crow)

    def direct(kind, u):
        return kind == "w" and u >= units - DIRECT

    def maybe(kind, u):
        return m > 1 and kind == "w" and units - DIRECT - EXTRA <= u < units - DIRECT

    def crossing(kind, u, yes, no):
        if direct(kind, u):
            yes()
        elif maybe(kind, u):
            pl.when(b + 1 < m)(yes)
            pl.when(b + 1 >= m)(no)
        else:
            no()

    def w_x(o, u, q=0):
        rows = w_rows(lax.rem(y + g - q, g), u)
        sems = (wx_s.at[o - 1, u], wx_r.at[o - 1, u])
        if q > 0:
            sems = (wy_s.at[o - 1, q - 1, u], wy_r.at[o - 1, q - 1, u])
        return remote(w_ref.at[rows], wfull.at[dp, rows], *sems, chip(lax.rem(x + o, nx), c))

    def w_y(o, q, u):
        ref = wfull.at[xs(o), w_rows(y, u)]
        return remote(
            ref, ref, wy_s.at[o - 1, q - 1, u], wy_r.at[o - 1, q - 1, u], {"grp": lax.rem(y + q, g)}
        )

    def w_c(o, q, u):
        ref = wfull.at[xs(o), w_rows(lax.rem(y + g - q, g), u)]
        return remote(ref, ref, wc_s.at[o - 1, q, u], wc_r.at[o - 1, q, u], partner)

    w_own = remote(w_ref, wfull.at[dp], wo_s, wo_r, partner)

    items = [("w", u) for u in range(units)]
    for f in range(pieces):
        for e in range(1, m):
            where = KEYS + (e - 1) * (units - KEYS) // (m - 1)
            items.insert(where + f * APART, ("k", (e, f)))
    for f in range(pieces):
        items.insert(1 + f, ("k", (0, f)))

    def issue(s):
        if s >= len(items):
            return
        kind, e = items[s]
        if kind == "k":
            e, f = e
            if e > 0 and f == 0:
                kz_copy(m - e, 0).wait_recv()

            @pl.when((b + e >= m) | (e == 0))
            def _():
                for o in range(1, nx):
                    k_x(o, (e, f)).start()

            if f == 0:
                for q in range(g if e == 0 else 1):
                    k_own(q, e).start()
        else:
            def more():
                for o in range(1, nx):
                    for q in range(1, g):
                        w_x(o, e, q).start()

            for o in range(1, nx):
                w_x(o, e).start()
            crossing(kind, e, more, lambda: None)

    def pass_x(s):
        if s >= len(items):
            return
        kind, e = items[s]
        in_x, in_y, in_c = (k_x, k_y, k_c) if kind == "k" else (w_x, w_y, w_c)
        if kind == "k" and e[0] > 0:
            @pl.when(b + e[0] >= m)
            def _():
                for o in range(1, nx):
                    k_x(o, e).wait_recv()

            @pl.when(b + e[0] < m)
            def _():
                for o in range(1, nx):
                    k_down(e[0], o, e[1]).wait_recv()
        else:
            for o in range(1, nx):
                in_x(o, e).wait_recv()

        def yes():
            for o in range(1, nx):
                in_c(o, 0, e).start()
                for q in range(1, g):
                    w_x(o, e, q).wait_recv()
                    in_c(o, q, e).start()

        def no():
            for o in range(1, nx):
                for q in range(1, g):
                    in_y(o, q, e).start()
                in_c(o, 0, e).start()

        crossing(kind, e, yes, no)
        if kind == "k" and e[0] == 0:
            for o in range(1, m):
                @pl.when(b - o >= 0)
                def _():
                    for d in range(1, nx):
                        k_down(o, d, e[1]).start()

    def pass_y(s):
        if s < 0 or s >= len(items):
            return
        kind, e = items[s]
        in_y, in_c = (k_y, k_c) if kind == "k" else (w_y, w_c)

        def no():
            for o in range(1, nx):
                for q in range(1, g):
                    in_y(o, q, e).wait_recv()
                    in_c(o, q, e).start()

        crossing(kind, e, lambda: None, no)

    def settle():
        for s in range(1, p):
            for copy in lat_mate(s):
                copy.wait_send()
        for o in range(1, m):
            @pl.when(b + o < m)
            def _():
                for copy in lat_group(o):
                    copy.wait_send()

            @pl.when(b - o >= 0)
            def _():
                for s in range(1, p):
                    for copy in lat_relay(o, s):
                        copy.wait_send()

            for q in range(g):
                kz_copy(o, q).wait_send()
        for e in range(m):
            for q in range(g):
                k_own(q, e).wait_send()
            for s in range(1, p):
                q_copy(s, e).wait_send()
        w_own.wait_send()

    def retire(s):
        if s < 0 or s >= len(items):
            return
        kind, e = items[s]
        in_x, in_y, in_c = (k_x, k_y, k_c) if kind == "k" else (w_x, w_y, w_c)
        if kind == "k" and e[0] > 0:
            @pl.when(b + e[0] >= m)
            def _():
                for o in range(1, nx):
                    k_x(o, e).wait_send()
        else:
            for o in range(1, nx):
                in_x(o, e).wait_send()
        if kind == "k" and e[0] == 0:
            for o in range(1, m):
                @pl.when(b - o >= 0)
                def _():
                    for d in range(1, nx):
                        k_down(o, d, e[1]).wait_send()

        def yes():
            for o in range(1, nx):
                for q in range(1, g):
                    w_x(o, e, q).wait_send()

        def no():
            for o in range(1, nx):
                for q in range(1, g):
                    in_y(o, q, e).wait_send()

        crossing(kind, e, yes, no)
        for o in range(1, nx):
            for q in range(g):
                in_c(o, q, e).wait_send()

    done = []
    total = len(items) + LAG

    def step():
        s = len(done)
        if s >= total:
            return
        done.append(s)
        if s == RELAY:
            relay()
            for e in range(1, m):
                for o in range(1, p):
                    q_copy(o, e).start()
        if s == LATE:
            late()
        issue(s + LEAD)
        pass_x(s)
        pass_y(s - LAG)
        retire(s - KEEP)

    along = beside if staged else (p - 1) + (m - 1)
    pl.semaphore_wait(barrier, along + (nx - 1) + (g - 1) + 1)
    if staged:
        greet(far)
    for s in range(LEAD):
        issue(s)

    get_lat.wait()
    get_gain.wait()
    latent = latin[...].astype(jnp.float32)
    square = jnp.mean(latent * latent, axis=-1, keepdims=True)
    lat[span(me * tok, tok), :] = (latent * lax.rsqrt(square + 1e-06) * gain[...]).astype(jnp.bfloat16)
    get_key.wait()
    get_table.wait()
    mine = span(r * tok, tok)
    first, second = turned(keyin[...], table[0, :, mine], table[1, :, mine])
    both = jnp.concatenate([first, second], axis=0).astype(jnp.bfloat16)
    for f in range(rope // rrows):
        rkey[me, :, f * tok : (f + 1) * tok] = both[f * rrows : (f + 1) * rrows]

    if staged:
        pl.semaphore_wait(far, beside)
    for o in range(1, m):
        kz_copy(o, 0).start()
    for o in range(1, m):
        @pl.when(b + o < m)
        def _():
            for copy in lat_group(o):
                copy.start()
    for s in range(1, p):
        for copy in lat_mate(s):
            copy.start()
    for o in range(1, m):
        for q in range(1, g):
            kz_copy(o, q).start()
    for s in range(1, p):
        q_copy(s, 0).start()
    w_own.start()

    for s in range(START):
        step()

    for s in range(1, p):
        for copy in lat_mate(s):
            copy.wait_recv()
    for o in range(1, m):
        @pl.when(b - o >= 0)
        def _():
            for s in range(1, p):
                for copy in lat_relay(o, s):
                    copy.wait_recv()

    @pl.loop(0, (b + 1) * p)
    def _(j):
        turn = jnp.concatenate(
            [rkey[j, :, f * tok : (f + 1) * tok] for f in range(rope // rrows)], axis=0
        ).astype(jnp.float32)
        filled = jnp.concatenate([turn, jnp.zeros((LANES - rope, tok), jnp.float32)], axis=0)
        shared[span(j * tok, tok), :] = filled.T.astype(jnp.bfloat16)

    variants = math.gcd(VARIANTS, m)
    stride = length // variants
    if stride > p * tok:
        @pl.loop((b + 1) * p, n)
        def _(j):
            rows = span(j * tok, tok)
            lat[rows, :] = jnp.zeros((tok, latw), lat.dtype)
            shared[rows, :] = jnp.zeros((tok, LANES), shared.dtype)

    def head_over(i, h, extent):
        row = lax.broadcasted_iota(jnp.int32, (stride, p * tok), 0)
        col = lax.broadcasted_iota(jnp.int32, (stride, p * tok), 1)
        kept = row - col <= b * (p * tok) - (extent - stride)
        both = jnp.dot(
            lat[:extent, :], kvw[i, :, h * wide : (h + 1) * wide], preferred_element_type=jnp.float32
        )
        keys = jnp.concatenate([both[:, :NOPE].astype(jnp.bfloat16), shared[:extent, :]], axis=1)
        values = both[:, NOPE:].T.astype(jnp.bfloat16)
        raw = jnp.concatenate([qbuf[t, i, h, :, :] for t in range(p)], axis=1)
        first, second = turned(raw[NOPE:], table[0], table[1])
        query = jnp.concatenate(
            [
                raw[:NOPE], first.astype(jnp.bfloat16), second.astype(jnp.bfloat16),
                jnp.zeros((LANES - rope, p * tok), jnp.bfloat16),
            ],
            axis=0,
        )
        s = jnp.dot(keys, query, preferred_element_type=jnp.float32)
        last = jnp.where(kept, s[extent - stride :], -jnp.inf)
        s = last if extent == stride else jnp.concatenate([s[: extent - stride], last], axis=0)
        top = jnp.max(s, axis=0, keepdims=True)
        e = jnp.exp2((s - top) * (scale * math.log2(math.e)))
        probs = (e * (1.0 / jnp.sum(e, axis=0, keepdims=True))).astype(jnp.bfloat16)
        o = jnp.dot(values, probs, preferred_element_type=jnp.float32)
        for t in range(p):
            attout[i, t, h] = o[:, t * tok : (t + 1) * tok].T.astype(jnp.bfloat16)

    def head(i, start):
        for v in range(variants):
            @pl.when(lax.div(b, m // variants) == v)
            def _():
                for h in range(start, min(start + HEADS, hn)):
                    head_over(i, h, (v + 1) * stride)

    def take_q(e):
        i = group(e)
        own_q(i).wait()
        for s in range(1, p):
            q_copy(s, e).wait_recv()

    def take_k(e):
        for q in range(g):
            k_own(q, e).wait_recv()
        for o in range(1, nx):
            for q in range(g):
                for f in range(pieces):
                    k_c(o, q, (e, f)).wait_recv()

    def attend(e, h):
        if h == 0:
            while e > 0 and len(done) <= items.index(("k", (e, pieces - 1))) + LAG:
                step()
            take_q(e)
            take_k(e)
        head(group(e), h)
        for k in range(h, min(h + HEADS, hn)):
            for s in range(1, p):
                a_copy(s, group(e), k).start()

    def project(k):
        while len(done) < min(len(items), items.index(("w", (k + 1) * sub - 1)) + 1) + LAG:
            step()
        if k == 0:
            own_w.wait()
            w_own.wait_recv()
        for u in range(k * sub, (k + 1) * sub):
            for o in range(1, nx):
                for q in range(g):
                    w_c(o, q, u).wait_recv()
        q, i = place(k)
        if k % p == 0:
            block = jnp.concatenate([attout[i, r, h] for h in range(hn)], axis=1)
        else:
            for h in range(hn):
                a_copy(p - k % p, i, h).wait_recv()
            block = jnp.concatenate([attin[q, i, h] for h in range(hn)], axis=1)
        rows = span((q + p * i) * kd, kd)
        for d in range(ndp):
            part_sum = jnp.dot(block, wfull[d, rows, :], preferred_element_type=jnp.float32)
            where = slice(d * cols, (d + 1) * cols)
            if k == 0:
                acc[:, where] = part_sum
            elif k < n - 1:
                acc[:, where] += part_sum
            else:
                out_ref[:, where] = (acc[:, where] + part_sum).astype(out_ref.dtype)

    own_k.wait()
    work = [functools.partial(project, k) for k in range(n)]
    if m * hn <= 2 * VARIANTS:
        work = [functools.partial(attend, e, h) for e in range(m) for h in range(0, hn, HEADS)] + work
    else:
        while len(done) < total:
            step()
        for e in range(m):
            take_q(e)
            take_k(e)

        @pl.loop(0, m)
        def _(e):
            i = lax.rem(b + e, m)
            for h in range(0, hn, HEADS):
                head(i, h)
            for h in range(hn):
                for s in range(1, p):
                    a_copy(s, i, h).start()

    for count in PLAN:
        for _ in range(min(count, len(work))):
            work.pop(0)()
        step()
    for piece in work[:-1]:
        piece()
    settle()
    work[-1]()
    while len(done) < total:
        step()

    for s in range(total - KEEP, len(items)):
        retire(s)
    for e in range(m):
        for s in range(1, p):
            for h in range(hn):
                a_copy(s, group(e), h).wait_send()


def body(sizes, queries, kv_latent, rope_key, kv_gain, kv_weight, out_weight):
    g, n, dp = sizes
    nx = dp // CORES
    tok, heads, width = queries.shape[1:]
    rope = width - NOPE
    hn = heads // n
    latw = kv_latent.shape[2]
    p = math.gcd(SPLIT, n)
    m = n // p
    sub = max(1, UNITS // n)
    units = n * sub
    q = jnp.transpose(queries[0], (1, 2, 0))
    key = jnp.transpose(rope_key[0])
    table = jnp.asarray(rotation_table(n * tok, rope))

    d_in, cols = out_weight.shape
    kcols = kv_weight.shape[1]
    dma = pltpu.SemaphoreType.DMA
    bf = jnp.bfloat16
    xn = max(nx - 1, 1)
    gn = max(g - 1, 1)
    pn = max(p - 1, 1)
    mn = max(m - 1, 1)
    vmem = pl.BlockSpec(memory_space=pltpu.VMEM)
    hbm = pl.BlockSpec(memory_space=pltpu.HBM)
    out = pl.pallas_call(
        functools.partial(kernel, n, g, nx, p, hn, rope, width**-0.5, sub),
        out_shape=pltpu.VMEM((tok, cols * dp), bf),
        in_specs=[hbm] * 7,
        out_specs=vmem,
        scratch_shapes=[
            pltpu.VMEM((p, m, hn, width, tok), bf),
            pltpu.VMEM((n * tok, latw), bf),
            pltpu.VMEM((n, rope * tok // latw, latw), bf),
            pltpu.VMEM((n * tok, LANES), bf),
            pltpu.VMEM((m, kv_weight.shape[0] * dp, kcols), bf),
            pltpu.VMEM((dp, d_in, cols), bf),
            pltpu.VMEM((m, p, hn, tok, VD), bf),
            pltpu.VMEM((p, m, hn, tok, VD), bf),
            pltpu.VMEM((tok, cols * dp), jnp.float32),
            pltpu.VMEM((tok, latw), bf),
            pltpu.VMEM((rope, tok), bf),
            pltpu.VMEM((1, latw), jnp.float32),
            pltpu.VMEM((2, rope // 2, p * tok), jnp.float32),
            dma((6 + m,)),
            dma((pn, 2)), dma((pn, 2)), dma((mn, 2)), dma((mn, 2)),
            dma((mn, pn, 2)), dma((mn, pn, 2)),
            dma((pn, m)), dma((pn, m)),
            dma((mn, g)), dma((mn, g)),
            dma((pn, m, hn)), dma((pn, m, hn)),
            dma((xn, m, PIECES)), dma((xn, m, PIECES)),
            dma((mn, xn, PIECES)), dma((mn, xn, PIECES)),
            dma((xn, gn, m, PIECES)), dma((xn, gn, m, PIECES)),
            dma((xn, g, m, PIECES)), dma((xn, g, m, PIECES)),
            dma((g, m)), dma((g, m)),
            dma((xn, units)), dma((xn, units)),
            dma((xn, gn, units)), dma((xn, gn, units)),
            dma((xn, g, units)), dma((xn, g, units)),
            dma(()), dma(()),
            pltpu.SemaphoreType.REGULAR,
        ],
        compiler_params=pltpu.CompilerParams(
            collective_id=0, has_side_effects=True, vmem_limit_bytes=60 * 1024 * 1024
        ),
    )(q, kv_latent[0], key, kv_gain[None], table, kv_weight, out_weight)
    return out[None]


def solution(mesh):
    sizes = (mesh.shape["grp"], mesh.shape["sp"], mesh.shape["dp"])
    return jax.shard_map(
        functools.partial(body, sizes),
        mesh=mesh,
        in_specs=(
            P(("grp", "dp"), "sp", None, None),
            P(("grp", "dp"), "sp", None),
            P(("grp", "dp"), "sp", None),
            P(),
            P("dp", "sp"),
            P(None, "dp"),
        ),
        out_specs=P(("grp", "dp"), "sp", None),
        check_vma=False,
    )
```

```python
import functools
import math

import jax
import jax.numpy as jnp
import numpy as np
from jax import lax
from jax.experimental import pallas as pl
from jax.experimental.pallas import tpu as pltpu
from jax.sharding import PartitionSpec as P

NOPE = 128
VD = 128
LANES = 128
CORES = 2
UNITS = 16
LEAD = 4
LAG = 4
KEYS = 8
RELAY = 9
LATE = 13
START = 14
DIRECT = 1
PIECES = 2
TILE = 16
APART = 1
EXTRA = 1
HEADS = 2
KEEP = 7
PLAN = (0, 1, 1, 0, 1, 1, 1, 1, 1)
SPLIT = 2
VARIANTS = 4
MESH = pl.DeviceIdType.MESH


def rotation_table(length, rope):
    half = rope // 2
    inverse = np.power(10000.0, -np.arange(half) * 2.0 / rope).astype(np.float32)
    angle = inverse[:, None] * np.arange(length, dtype=np.float32)[None, :]
    return np.stack([np.cos(angle), np.sin(angle)]).astype(np.float32)


def kernel(
    n, g, nx, p, hn, rope, scale, sub,
    q_ref, latent_ref, key_ref, gain_ref, table_ref, kvw_ref, w_ref, out_ref,
    qbuf, lat, rkey, shared, kvw, wfull, attout, attin, acc, latin, keyin, gain, table,
    loc, lm_s, lm_r, lg_s, lg_r, lr_s, lr_r, q_s, q_r, kz_s, kz_r, a_s, a_r,
    kx_s, kx_r, kf_s, kf_r, ky_s, ky_r, kc_s, kc_r, ko_s, ko_r,
    wx_s, wx_r, wy_s, wy_r, wc_s, wc_r, wo_s, wo_r, far,
):
    me = lax.axis_index("sp")
    y = lax.axis_index("grp")
    dp = lax.axis_index("dp")
    x, c = dp // CORES, dp % CORES
    b, r = lax.div(me, p), lax.rem(me, p)
    m = n // p
    ndp = nx * CORES
    tok, latw = latent_ref.shape
    half = rope // 2
    rrows = rkey.shape[1]
    krows = kvw_ref.shape[0]
    kh = krows // g
    pieces = math.gcd(PIECES, max(1, kh // TILE))
    ks = kh // pieces
    cols = w_ref.shape[1]
    kd = hn * VD
    part = kd // g
    crow = part // sub
    units = n * sub
    length = n * tok
    wide = NOPE + VD

    def chip(xx, cc):
        return {"dp": xx * CORES + cc}

    partner = chip(x, 1 - c)

    def remote(src, dst, ss, rs, dev):
        return pltpu.make_async_remote_copy(
            src_ref=src, dst_ref=dst, send_sem=ss, recv_sem=rs, device_id=dev, device_id_type=MESH
        )

    def span(start, size):
        return pl.ds(pl.multiple_of(start, size), size)

    def mate(s):
        return lax.rem(r + s, p)

    def group(o):
        return lax.rem(b + o, m)

    def xs(o):
        return lax.rem(x + nx - o, nx) * CORES + c

    get_lat = pltpu.make_async_copy(latent_ref, latin, loc.at[0])
    get_key = pltpu.make_async_copy(key_ref, keyin, loc.at[1])
    get_gain = pltpu.make_async_copy(gain_ref, gain, loc.at[2])
    get_table = pltpu.make_async_copy(table_ref.at[:, :, span(b * (p * tok), p * tok)], table, loc.at[3])
    own_k = pltpu.make_async_copy(kvw_ref, kvw.at[b, span(dp * krows, krows)], loc.at[4])
    own_w = pltpu.make_async_copy(w_ref, wfull.at[dp], loc.at[5])

    def own_q(i):
        return pltpu.make_async_copy(q_ref.at[span((r + p * i) * hn, hn)], qbuf.at[r, i], loc.at[6 + i])

    for copy in (get_lat, get_key, get_gain, get_table):
        copy.start()

    barrier = pltpu.get_barrier_semaphore()
    staged = (m - 1) * p == 2

    def greet(semaphore):
        @pl.when(me > 0)
        def _():
            pl.semaphore_signal(semaphore, 1, device_id={"sp": me - 1}, device_id_type=MESH)

        @pl.when(me < n - 1)
        def _():
            pl.semaphore_signal(semaphore, 1, device_id={"sp": me + 1}, device_id_type=MESH)

    beside = jnp.where(me > 0, 1, 0) + jnp.where(me < n - 1, 1, 0)
    if staged:
        greet(barrier)
    else:
        for s in range(1, p):
            pl.semaphore_signal(barrier, 1, device_id={"sp": b * p + mate(s)}, device_id_type=MESH)
        for o in range(1, m):
            pl.semaphore_signal(barrier, 1, device_id={"sp": group(o) * p + r}, device_id_type=MESH)
    for o in range(1, nx):
        pl.semaphore_signal(barrier, 1, device_id=chip(lax.rem(x + o, nx), c), device_id_type=MESH)
    for o in range(1, g):
        pl.semaphore_signal(barrier, 1, device_id={"grp": lax.rem(y + o, g)}, device_id_type=MESH)
    pl.semaphore_signal(barrier, 1, device_id=partner, device_id_type=MESH)

    own_k.start()
    for i in range(m):
        own_q(i).start()
    own_w.start()

    def turned(values, cosine, sine):
        first, second = values[:half].astype(jnp.float32), values[half:].astype(jnp.float32)
        return first * cosine - second * sine, first * sine + second * cosine

    def kz_copy(o, q):
        part_of = lax.rem(y + q, g)
        return remote(
            kvw_ref.at[span(part_of * kh, kh)], k_rows(b, dp, part_of),
            kz_s.at[o - 1, q], kz_r.at[o - 1, q], {"sp": group(o) * p + r},
        )

    def lat_pair(j, to, ss, rs):
        rows = span(j * tok, tok)
        return (
            remote(lat.at[rows], lat.at[rows], ss.at[0], rs.at[0], {"sp": to}),
            remote(rkey.at[j], rkey.at[j], ss.at[1], rs.at[1], {"sp": to}),
        )

    def lat_mate(s):
        return lat_pair(me, b * p + mate(s), lm_s.at[s - 1], lm_r.at[s - 1])

    def lat_group(o):
        return lat_pair(me, group(o) * p + r, lg_s.at[o - 1], lg_r.at[o - 1])

    def lat_relay(o, s):
        j = lax.rem(b + m - o, m) * p + r
        return lat_pair(j, b * p + mate(s), lr_s.at[o - 1, s - 1], lr_r.at[o - 1, s - 1])

    def relay():
        for o in range(1, m):
            @pl.when(b - o >= 0)
            def _():
                for copy in lat_group(o):
                    copy.wait_recv()
                for s in range(1, p):
                    for copy in lat_relay(o, s):
                        copy.start()

    def q_copy(s, e):
        t, i = mate(s), group(e)
        return remote(
            q_ref.at[span((t + p * i) * hn, hn)], qbuf.at[r, i], q_s.at[s - 1, i], q_r.at[s - 1, i],
            {"sp": b * p + t},
        )

    def a_copy(s, i, h):
        t = mate(s)
        return remote(
            attout.at[i, t, h], attin.at[r, i, h], a_s.at[s - 1, i, h], a_r.at[s - 1, i, h],
            {"sp": b * p + t},
        )

    def k_rows(i, d, q):
        return kvw.at[i, span(d * krows + q * kh, kh)]

    def k_piece(i, d, q, f):
        return kvw.at[i, pl.ds(pl.multiple_of(d * krows + q * kh + f * ks, TILE), ks)]

    def k_x(o, ef):
        e, f = ef
        dst = k_piece(group(e), dp, y, f)
        src = kvw_ref.at[pl.ds(pl.multiple_of(y * kh + f * ks, TILE), ks)] if e == 0 else dst
        return remote(
            src, dst, kx_s.at[o - 1, e, f], kx_r.at[o - 1, e, f], chip(lax.rem(x + o, nx), c)
        )

    def k_down(s, o, f):
        ref = k_piece(b, xs(o), y, f)
        return remote(
            ref, ref, kf_s.at[s - 1, o - 1, f], kf_r.at[s - 1, o - 1, f],
            {"sp": lax.rem(b + m - s, m) * p + r},
        )

    def k_y(o, q, ef):
        e, f = ef
        ref = k_piece(group(e), xs(o), y, f)
        return remote(
            ref, ref, ky_s.at[o - 1, q - 1, e, f], ky_r.at[o - 1, q - 1, e, f],
            {"grp": lax.rem(y + q, g)},
        )

    def k_c(o, q, ef):
        e, f = ef
        ref = k_piece(group(e), xs(o), lax.rem(y + g - q, g), f)
        return remote(ref, ref, kc_s.at[o - 1, q, e, f], kc_r.at[o - 1, q, e, f], partner)

    def k_own(q, e):
        part_of = lax.rem(y + q, g)
        dst = k_rows(group(e), dp, part_of)
        src = kvw_ref.at[span(part_of * kh, kh)] if e == 0 else dst
        return remote(src, dst, ko_s.at[q, e], ko_r.at[q, e], partner)

    def late():
        for e in range(1, m):
            for q in range(1, g):
                kz_copy(m - e, q).wait_recv()
                k_own(q, e).start()

    def place(k):
        return lax.rem(r + k % p, p), group(k // p)

    def w_rows(yy, u):
        q, i = place(u // sub)
        return span((q + p * i) * kd + yy * part + (u % sub) * crow, crow)

    def direct(kind, u):
        return kind == "w" and u >= units - DIRECT

    def maybe(kind, u):
        return m > 1 and kind == "w" and units - DIRECT - EXTRA <= u < units - DIRECT

    def crossing(kind, u, yes, no):
        if direct(kind, u):
            yes()
        elif maybe(kind, u):
            pl.when(b + 1 < m)(yes)
            pl.when(b + 1 >= m)(no)
        else:
            no()

    def w_x(o, u, q=0):
        rows = w_rows(lax.rem(y + g - q, g), u)
        sems = (wx_s.at[o - 1, u], wx_r.at[o - 1, u])
        if q > 0:
            sems = (wy_s.at[o - 1, q - 1, u], wy_r.at[o - 1, q - 1, u])
        return remote(w_ref.at[rows], wfull.at[dp, rows], *sems, chip(lax.rem(x + o, nx), c))

    def w_y(o, q, u):
        ref = wfull.at[xs(o), w_rows(y, u)]
        return remote(
            ref, ref, wy_s.at[o - 1, q - 1, u], wy_r.at[o - 1, q - 1, u], {"grp": lax.rem(y + q, g)}
        )

    def w_c(o, q, u):
        ref = wfull.at[xs(o), w_rows(lax.rem(y + g - q, g), u)]
        return remote(ref, ref, wc_s.at[o - 1, q, u], wc_r.at[o - 1, q, u], partner)

    w_own = remote(w_ref, wfull.at[dp], wo_s, wo_r, partner)

    items = [("w", u) for u in range(units)]
    for f in range(pieces):
        for e in range(1, m):
            where = KEYS + (e - 1) * (units - KEYS) // (m - 1)
            items.insert(where + f * APART, ("k", (e, f)))
    for f in range(pieces):
        items.insert(1 + f, ("k", (0, f)))

    def issue(s):
        if s >= len(items):
            return
        kind, e = items[s]
        if kind == "k":
            e, f = e
            if e > 0 and f == 0:
                kz_copy(m - e, 0).wait_recv()

            @pl.when((b + e >= m) | (e == 0))
            def _():
                for o in range(1, nx):
                    k_x(o, (e, f)).start()

            if f == 0:
                for q in range(g if e == 0 else 1):
                    k_own(q, e).start()
        else:
            def more():
                for o in range(1, nx):
                    for q in range(1, g):
                        w_x(o, e, q).start()

            for o in range(1, nx):
                w_x(o, e).start()
            crossing(kind, e, more, lambda: None)

    def pass_x(s):
        if s >= len(items):
            return
        kind, e = items[s]
        in_x, in_y, in_c = (k_x, k_y, k_c) if kind == "k" else (w_x, w_y, w_c)
        if kind == "k" and e[0] > 0:
            @pl.when(b + e[0] >= m)
            def _():
                for o in range(1, nx):
                    k_x(o, e).wait_recv()

            @pl.when(b + e[0] < m)
            def _():
                for o in range(1, nx):
                    k_down(e[0], o, e[1]).wait_recv()
        else:
            for o in range(1, nx):
                in_x(o, e).wait_recv()

        def yes():
            for o in range(1, nx):
                in_c(o, 0, e).start()
                for q in range(1, g):
                    w_x(o, e, q).wait_recv()
                    in_c(o, q, e).start()

        def no():
            for o in range(1, nx):
                for q in range(1, g):
                    in_y(o, q, e).start()
                in_c(o, 0, e).start()

        crossing(kind, e, yes, no)
        if kind == "k" and e[0] == 0:
            for o in range(1, m):
                @pl.when(b - o >= 0)
                def _():
                    for d in range(1, nx):
                        k_down(o, d, e[1]).start()

    def pass_y(s):
        if s < 0 or s >= len(items):
            return
        kind, e = items[s]
        in_y, in_c = (k_y, k_c) if kind == "k" else (w_y, w_c)

        def no():
            for o in range(1, nx):
                for q in range(1, g):
                    in_y(o, q, e).wait_recv()
                    in_c(o, q, e).start()

        crossing(kind, e, lambda: None, no)

    def settle():
        for s in range(1, p):
            for copy in lat_mate(s):
                copy.wait_send()
        for o in range(1, m):
            @pl.when(b + o < m)
            def _():
                for copy in lat_group(o):
                    copy.wait_send()

            @pl.when(b - o >= 0)
            def _():
                for s in range(1, p):
                    for copy in lat_relay(o, s):
                        copy.wait_send()

            for q in range(g):
                kz_copy(o, q).wait_send()
        for e in range(m):
            for q in range(g):
                k_own(q, e).wait_send()
            for s in range(1, p):
                q_copy(s, e).wait_send()
        w_own.wait_send()

    def retire(s):
        if s < 0 or s >= len(items):
            return
        kind, e = items[s]
        in_x, in_y, in_c = (k_x, k_y, k_c) if kind == "k" else (w_x, w_y, w_c)
        if kind == "k" and e[0] > 0:
            @pl.when(b + e[0] >= m)
            def _():
                for o in range(1, nx):
                    k_x(o, e).wait_send()
        else:
            for o in range(1, nx):
                in_x(o, e).wait_send()
        if kind == "k" and e[0] == 0:
            for o in range(1, m):
                @pl.when(b - o >= 0)
                def _():
                    for d in range(1, nx):
                        k_down(o, d, e[1]).wait_send()

        def yes():
            for o in range(1, nx):
                for q in range(1, g):
                    w_x(o, e, q).wait_send()

        def no():
            for o in range(1, nx):
                for q in range(1, g):
                    in_y(o, q, e).wait_send()

        crossing(kind, e, yes, no)
        for o in range(1, nx):
            for q in range(g):
                in_c(o, q, e).wait_send()

    done = []
    total = len(items) + LAG

    def step():
        s = len(done)
        if s >= total:
            return
        done.append(s)
        if s == RELAY:
            relay()
            for e in range(1, m):
                for o in range(1, p):
                    q_copy(o, e).start()
        if s == LATE:
            late()
        issue(s + LEAD)
        pass_y(s - LAG)
        pass_x(s)
        retire(s - KEEP)

    along = beside if staged else (p - 1) + (m - 1)
    pl.semaphore_wait(barrier, along + (nx - 1) + (g - 1) + 1)
    if staged:
        greet(far)
    for s in range(LEAD):
        issue(s)

    get_lat.wait()
    get_gain.wait()
    latent = latin[...].astype(jnp.float32)
    square = jnp.mean(latent * latent, axis=-1, keepdims=True)
    lat[span(me * tok, tok), :] = (latent * lax.rsqrt(square + 1e-06) * gain[...]).astype(jnp.bfloat16)
    get_key.wait()
    get_table.wait()
    mine = span(r * tok, tok)
    first, second = turned(keyin[...], table[0, :, mine], table[1, :, mine])
    both = jnp.concatenate([first, second], axis=0).astype(jnp.bfloat16)
    for f in range(rope // rrows):
        rkey[me, :, f * tok : (f + 1) * tok] = both[f * rrows : (f + 1) * rrows]

    if staged:
        pl.semaphore_wait(far, beside)
    for o in range(1, m):
        kz_copy(o, 0).start()
    for o in range(1, m):
        @pl.when(b + o < m)
        def _():
            for copy in lat_group(o):
                copy.start()
    for s in range(1, p):
        for copy in lat_mate(s):
            copy.start()
    for o in range(1, m):
        for q in range(1, g):
            kz_copy(o, q).start()
    for s in range(1, p):
        q_copy(s, 0).start()
    w_own.start()

    for s in range(START):
        step()

    for s in range(1, p):
        for copy in lat_mate(s):
            copy.wait_recv()
    for o in range(1, m):
        @pl.when(b - o >= 0)
        def _():
            for s in range(1, p):
                for copy in lat_relay(o, s):
                    copy.wait_recv()

    @pl.loop(0, (b + 1) * p)
    def _(j):
        turn = jnp.concatenate(
            [rkey[j, :, f * tok : (f + 1) * tok] for f in range(rope // rrows)], axis=0
        ).astype(jnp.float32)
        filled = jnp.concatenate([turn, jnp.zeros((LANES - rope, tok), jnp.float32)], axis=0)
        shared[span(j * tok, tok), :] = filled.T.astype(jnp.bfloat16)

    variants = math.gcd(VARIANTS, m)
    stride = length // variants
    if stride > p * tok:
        @pl.loop((b + 1) * p, n)
        def _(j):
            rows = span(j * tok, tok)
            lat[rows, :] = jnp.zeros((tok, latw), lat.dtype)
            shared[rows, :] = jnp.zeros((tok, LANES), shared.dtype)

    def head_over(i, h, extent):
        row = lax.broadcasted_iota(jnp.int32, (stride, p * tok), 0)
        col = lax.broadcasted_iota(jnp.int32, (stride, p * tok), 1)
        kept = row - col <= b * (p * tok) - (extent - stride)
        both = jnp.dot(
            lat[:extent, :], kvw[i, :, h * wide : (h + 1) * wide], preferred_element_type=jnp.float32
        )
        keys = jnp.concatenate([both[:, :NOPE].astype(jnp.bfloat16), shared[:extent, :]], axis=1)
        values = both[:, NOPE:].T.astype(jnp.bfloat16)
        raw = jnp.concatenate([qbuf[t, i, h, :, :] for t in range(p)], axis=1)
        first, second = turned(raw[NOPE:], table[0], table[1])
        query = jnp.concatenate(
            [
                raw[:NOPE], first.astype(jnp.bfloat16), second.astype(jnp.bfloat16),
                jnp.zeros((LANES - rope, p * tok), jnp.bfloat16),
            ],
            axis=0,
        )
        s = jnp.dot(keys, query, preferred_element_type=jnp.float32)
        last = jnp.where(kept, s[extent - stride :], -jnp.inf)
        s = last if extent == stride else jnp.concatenate([s[: extent - stride], last], axis=0)
        top = jnp.max(s, axis=0, keepdims=True)
        e = jnp.exp2((s - top) * (scale * math.log2(math.e)))
        probs = (e * (1.0 / jnp.sum(e, axis=0, keepdims=True))).astype(jnp.bfloat16)
        o = jnp.dot(values, probs, preferred_element_type=jnp.float32)
        for t in range(p):
            attout[i, t, h] = o[:, t * tok : (t + 1) * tok].T.astype(jnp.bfloat16)

    def head(i, start):
        for v in range(variants):
            @pl.when(lax.div(b, m // variants) == v)
            def _():
                for h in range(start, min(start + HEADS, hn)):
                    head_over(i, h, (v + 1) * stride)

    def take_q(e):
        i = group(e)
        own_q(i).wait()
        for s in range(1, p):
            q_copy(s, e).wait_recv()

    def take_k(e):
        for q in range(g):
            k_own(q, e).wait_recv()
        for o in range(1, nx):
            for q in range(g):
                for f in range(pieces):
                    k_c(o, q, (e, f)).wait_recv()

    def attend(e, h):
        if h == 0:
            while e > 0 and len(done) <= items.index(("k", (e, pieces - 1))) + LAG:
                step()
            take_q(e)
            take_k(e)
        head(group(e), h)
        for k in range(h, min(h + HEADS, hn)):
            for s in range(1, p):
                a_copy(s, group(e), k).start()

    def project(k):
        while len(done) < min(len(items), items.index(("w", (k + 1) * sub - 1)) + 1) + LAG:
            step()
        if k == 0:
            own_w.wait()
            w_own.wait_recv()
        for u in range(k * sub, (k + 1) * sub):
            for o in range(1, nx):
                for q in range(g):
                    w_c(o, q, u).wait_recv()
        q, i = place(k)
        if k % p == 0:
            block = jnp.concatenate([attout[i, r, h] for h in range(hn)], axis=1)
        else:
            for h in range(hn):
                a_copy(p - k % p, i, h).wait_recv()
            block = jnp.concatenate([attin[q, i, h] for h in range(hn)], axis=1)
        rows = span((q + p * i) * kd, kd)
        for d in range(ndp):
            part_sum = jnp.dot(block, wfull[d, rows, :], preferred_element_type=jnp.float32)
            where = slice(d * cols, (d + 1) * cols)
            if k == 0:
                acc[:, where] = part_sum
            elif k < n - 1:
                acc[:, where] += part_sum
            else:
                out_ref[:, where] = (acc[:, where] + part_sum).astype(out_ref.dtype)

    own_k.wait()
    work = [functools.partial(project, k) for k in range(n)]
    if m * hn <= 2 * VARIANTS:
        work = [functools.partial(attend, e, h) for e in range(m) for h in range(0, hn, HEADS)] + work
    else:
        while len(done) < total:
            step()
        for e in range(m):
            take_q(e)
            take_k(e)

        @pl.loop(0, m)
        def _(e):
            i = lax.rem(b + e, m)
            for h in range(0, hn, HEADS):
                head(i, h)
            for h in range(hn):
                for s in range(1, p):
                    a_copy(s, i, h).start()

    for count in PLAN:
        for _ in range(min(count, len(work))):
            work.pop(0)()
        step()
    for piece in work[:-1]:
        piece()
    settle()
    work[-1]()
    while len(done) < total:
        step()

    for s in range(total - KEEP, len(items)):
        retire(s)
    for e in range(m):
        for s in range(1, p):
            for h in range(hn):
                a_copy(s, group(e), h).wait_send()


def body(sizes, queries, kv_latent, rope_key, kv_gain, kv_weight, out_weight):
    g, n, dp = sizes
    nx = dp // CORES
    tok, heads, width = queries.shape[1:]
    rope = width - NOPE
    hn = heads // n
    latw = kv_latent.shape[2]
    p = math.gcd(SPLIT, n)
    m = n // p
    sub = max(1, UNITS // n)
    units = n * sub
    q = jnp.transpose(queries[0], (1, 2, 0))
    key = jnp.transpose(rope_key[0])
    table = jnp.asarray(rotation_table(n * tok, rope))

    d_in, cols = out_weight.shape
    kcols = kv_weight.shape[1]
    dma = pltpu.SemaphoreType.DMA
    bf = jnp.bfloat16
    xn = max(nx - 1, 1)
    gn = max(g - 1, 1)
    pn = max(p - 1, 1)
    mn = max(m - 1, 1)
    vmem = pl.BlockSpec(memory_space=pltpu.VMEM)
    hbm = pl.BlockSpec(memory_space=pltpu.HBM)
    out = pl.pallas_call(
        functools.partial(kernel, n, g, nx, p, hn, rope, width**-0.5, sub),
        out_shape=pltpu.VMEM((tok, cols * dp), bf),
        in_specs=[hbm] * 7,
        out_specs=vmem,
        scratch_shapes=[
            pltpu.VMEM((p, m, hn, width, tok), bf),
            pltpu.VMEM((n * tok, latw), bf),
            pltpu.VMEM((n, rope * tok // latw, latw), bf),
            pltpu.VMEM((n * tok, LANES), bf),
            pltpu.VMEM((m, kv_weight.shape[0] * dp, kcols), bf),
            pltpu.VMEM((dp, d_in, cols), bf),
            pltpu.VMEM((m, p, hn, tok, VD), bf),
            pltpu.VMEM((p, m, hn, tok, VD), bf),
            pltpu.VMEM((tok, cols * dp), jnp.float32),
            pltpu.VMEM((tok, latw), bf),
            pltpu.VMEM((rope, tok), bf),
            pltpu.VMEM((1, latw), jnp.float32),
            pltpu.VMEM((2, rope // 2, p * tok), jnp.float32),
            dma((6 + m,)),
            dma((pn, 2)), dma((pn, 2)), dma((mn, 2)), dma((mn, 2)),
            dma((mn, pn, 2)), dma((mn, pn, 2)),
            dma((pn, m)), dma((pn, m)),
            dma((mn, g)), dma((mn, g)),
            dma((pn, m, hn)), dma((pn, m, hn)),
            dma((xn, m, PIECES)), dma((xn, m, PIECES)),
            dma((mn, xn, PIECES)), dma((mn, xn, PIECES)),
            dma((xn, gn, m, PIECES)), dma((xn, gn, m, PIECES)),
            dma((xn, g, m, PIECES)), dma((xn, g, m, PIECES)),
            dma((g, m)), dma((g, m)),
            dma((xn, units)), dma((xn, units)),
            dma((xn, gn, units)), dma((xn, gn, units)),
            dma((xn, g, units)), dma((xn, g, units)),
            dma(()), dma(()),
            pltpu.SemaphoreType.REGULAR,
        ],
        compiler_params=pltpu.CompilerParams(
            collective_id=0, has_side_effects=True, vmem_limit_bytes=60 * 1024 * 1024
        ),
    )(q, kv_latent[0], key, kv_gain[None], table, kv_weight, out_weight)
    return out[None]


def solution(mesh):
    sizes = (mesh.shape["grp"], mesh.shape["sp"], mesh.shape["dp"])
    return jax.shard_map(
        functools.partial(body, sizes),
        mesh=mesh,
        in_specs=(
            P(("grp", "dp"), "sp", None, None),
            P(("grp", "dp"), "sp", None),
            P(("grp", "dp"), "sp", None),
            P(),
            P("dp", "sp"),
            P(None, "dp"),
        ),
        out_specs=P(("grp", "dp"), "sp", None),
        check_vma=False,
    )
```
